32 devices in a mesh: sp: 16 (over z, y, x), tp: 2 (over core).
Axes of the slice: x: 2, y: 2, z: 4, core: 2. Of those that a mesh axis runs over, the one named last changes fastest.
Arguments:
- resid: bfloat16 [3072, 2048], P(('sp', 'tp')), may hold values from -6 to 6
- queries: bfloat16 [3072, 2048], P('sp', 'tp'), may hold values from -8 to 8
- keys: bfloat16 [3072, 512], P('sp', 'tp'), may hold values from -8 to 8
- values: bfloat16 [3072, 512], P('sp', 'tp'), may hold values from -6 to 6
- log_gates: float32 [3072, 32], P('sp', 'tp'), may hold values from -1536 to 0, as said below
- out_gate: bfloat16 [3072, 2048], P('sp', 'tp'), may hold values from -8 to 8
- out_weight: bfloat16 [2048, 2048], P('tp'), may hold values from -0.125 to 0.125
- post_gain: float32 [2048], replicated, may hold values from 0.1 to 1.9
- pre_gain: float32 [2048], replicated, may hold values from 0.1 to 1.9
- ffn_gain: float32 [2048], replicated, may hold values from 0.1 to 1.9
- gate_weight: bfloat16 [2048, 5632], P('sp', 'tp'), may hold values from -0.125 to 0.125
- up_weight: bfloat16 [2048, 5632], P('sp', 'tp'), may hold values from -0.125 to 0.125
- down_weight: bfloat16 [5632, 2048], P('tp', 'sp'), may hold values from -0.078125 to 0.078125
Outputs:
- result: bfloat16 [3072, 2048], P(('sp', 'tp'))
The draws below stay inside these ranges and needn't reach their ends.
Inputs may be any that keep to these rules, and one draw needn't show every extreme that they name: Each head's column of log_gates never rises from one position to the next, and its first entry is at most 0.
All inputs are finite; a program needn't handle non-finite values.
Results may differ from the reference program's by a relative error of at most 0.017.
Values may be sent and summed in bfloat16 or wider, within the bound.
A program may use at most 128 MiB of HBM per device.

```python
import math
import jax
import jax.numpy as jnp
from jax import lax

D = 2048
H = 32
KV = 8
HD = 64
FF = 5632
TOK_DEV = 192
TOKENS = 3072


def base_field(key, shape):
    return jnp.clip(jax.random.normal(key, shape, jnp.float32), -4.0, 4.0)


def draw_queries(key, part):
    field = base_field(jax.random.fold_in(key, 11), (TOKENS, H * HD))
    return field.astype(jnp.bfloat16)


def draw_keys(key, part):
    field = base_field(jax.random.fold_in(key, 13), (TOKENS, KV * HD))
    return field.astype(jnp.bfloat16)


def draw_log_gates(key, part):
    keyring = jax.random.split(jax.random.fold_in(key, 17), 5)
    order = jax.random.permutation(keyring[0], H)
    slow = order >= H // 2
    rate = jnp.where(slow, 0.5 / TOKENS, 1.0 / 40.0).astype(jnp.float32)
    blocks = TOKENS // TOK_DEV
    block_factor = jnp.exp(jax.random.uniform(keyring[1], (blocks,), jnp.float32, math.log(0.4), math.log(2.5)))
    block_factor = jnp.repeat(block_factor, TOK_DEV)[:, None]
    data = jnp.exp(0.6 * jnp.clip(jax.random.normal(keyring[2], (TOKENS, H), jnp.float32), -3.0, 3.0))
    steps = -rate[None, :] * block_factor * data
    hits = jax.random.uniform(keyring[3], (TOKENS, H), jnp.float32) < 2.0 / TOKENS
    loss = jax.random.uniform(keyring[4], (TOKENS, H), jnp.float32, 0.2, 0.5)
    steps = steps + jnp.where(hits & slow[None, :], jnp.log(1.0 - loss), 0.0)
    return jnp.cumsum(steps, axis=0).astype(jnp.float32)


def block_scale(rng, extent, cuts, least, top_value):
    def one(dim, shards_of):
        draws = jax.random.uniform(jax.random.fold_in(jax.random.fold_in(rng, 6), dim), (shards_of,), jnp.float32, least / len(cuts), top_value / len(cuts))
        return jnp.repeat(jnp.exp(draws), extent[dim] // shards_of).reshape((-1,) + (1,) * (len(extent) - dim - 1))

    level = one(*cuts[0])
    for cut in cuts[1:]:
        level = level * one(*cut)
    return level


def centred(own_key, extent, deviation, reach, cuts=(), kind=jnp.bfloat16):
    level = block_scale(own_key, extent, cuts, -0.22, 0.18) if cuts else 1.0
    entries = jax.random.normal(own_key, extent, jnp.float32) * deviation * level
    return jnp.minimum(jnp.maximum(entries, -reach), reach).astype(kind)


def setup_inputs(seed: int = 0) -> dict:
    seeds = jax.random.split(jax.random.key(seed), 14)
    return {
        "resid": centred(seeds[0], (TOKENS, D), 1.0, 6.0, ((0, 32),)),
        "queries": draw_queries(jax.random.fold_in(seeds[13], 71), 0),
        "keys": draw_keys(jax.random.fold_in(seeds[13], 71), 0),
        "values": centred(seeds[3], (TOKENS, KV * HD), 1.0, 6.0, ((0, 16), (1, 2))),
        "log_gates": draw_log_gates(jax.random.fold_in(seeds[13], 71), 0),
        "out_gate": centred(seeds[5], (TOKENS, H * HD), 1.5, 8.0, ((0, 16), (1, 2))),
        "out_weight": centred(seeds[6], (H * HD, D), (H * HD) ** -0.5, 0.125, ((0, 2),)),
        "post_gain": jnp.clip(1.0 + 0.18 * jax.random.normal(seeds[7], (D,), jnp.float32), 0.1, 1.9),
        "pre_gain": jnp.clip(1.0 + 0.18 * jax.random.normal(seeds[8], (D,), jnp.float32), 0.1, 1.9),
        "ffn_gain": jnp.clip(1.0 + 0.18 * jax.random.normal(seeds[9], (D,), jnp.float32), 0.1, 1.9),
        "gate_weight": centred(seeds[10], (D, FF), D ** -0.5, 0.125, ((0, 16), (1, 2))),
        "up_weight": centred(seeds[11], (D, FF), D ** -0.5, 0.125, ((0, 16), (1, 2))),
        "down_weight": centred(seeds[12], (FF, D), FF ** -0.5, 0.078125, ((0, 2), (1, 16))),
    }


EPS = 1e-06
QUERY_BLOCK = 512

def rms_scale(rows, gain):
    mean_sq = lax.optimization_barrier(jnp.mean(rows * rows, axis=-1, keepdims=True))
    return rows * lax.rsqrt(mean_sq + EPS) * gain

def reference(resid, queries, keys, values, log_gates, out_gate, out_weight, post_gain, pre_gain, ffn_gain, gate_weight, up_weight, down_weight):
    group = H // KV
    scale = HD ** (-0.5)
    total = queries.shape[0]

    def one_head(head):
        kv_head = head // group
        q_head = lax.dynamic_slice_in_dim(queries, (head * HD).astype(jnp.int32), HD, 1)
        k_head = lax.dynamic_slice_in_dim(keys, (kv_head * HD).astype(jnp.int32), HD, 1)
        v_head = lax.dynamic_slice_in_dim(values, (kv_head * HD).astype(jnp.int32), HD, 1)
        c_head = lax.dynamic_slice_in_dim(log_gates, head.astype(jnp.int32), 1, 1)[:, 0]
        pieces = []
        for first in range(0, total, QUERY_BLOCK):
            end = min(first + QUERY_BLOCK, total)
            count = end - first
            scores = jnp.dot(q_head[first:end], k_head[:end].T, preferred_element_type=jnp.float32) * scale
            scores = scores + c_head[first:end, None] - c_head[None, :end]
            causal = (first + jnp.arange(count))[:, None] >= jnp.arange(end)[None, :]
            scores = jnp.where(causal, scores, -jnp.inf)
            top = lax.optimization_barrier(jnp.max(scores, axis=1, keepdims=True))
            weights = jnp.exp(scores - top)
            denom = lax.optimization_barrier(jnp.sum(weights, axis=1, keepdims=True))
            pieces.append(jnp.dot(weights.astype(jnp.bfloat16), v_head[:end], preferred_element_type=jnp.float32) / denom)
        return jnp.concatenate(pieces, axis=0)
    attended = lax.map(one_head, jnp.arange(H, dtype=jnp.int32))
    attended = attended.transpose(1, 0, 2).reshape(total, H * HD)
    gated = (attended * jax.nn.sigmoid(out_gate.astype(jnp.float32))).astype(jnp.bfloat16)
    projected = jnp.dot(gated, out_weight, preferred_element_type=jnp.float32)
    mixed = resid.astype(jnp.float32) + rms_scale(projected, post_gain)
    normed = rms_scale(mixed, pre_gain).astype(jnp.bfloat16)
    gate = jnp.dot(normed, gate_weight, preferred_element_type=jnp.float32)
    up = jnp.dot(normed, up_weight, preferred_element_type=jnp.float32)
    hidden = (jax.nn.silu(gate) * up).astype(jnp.bfloat16)
    ffn = jnp.dot(hidden, down_weight, preferred_element_type=jnp.float32)
    return (mixed + rms_scale(ffn, ffn_gain)).astype(jnp.bfloat16)
```

```python
import jax
import jax.numpy as jnp
from jax import lax
from jax.experimental import pallas as pl
from jax.experimental.pallas import tpu as pltpu
from jax.sharding import PartitionSpec as P

HD = 64


EPS = 1e-06
KEY_BLOCK = 512


def rms_scale(rows, gain):
    mean_sq = jnp.mean(rows * rows, axis=-1, keepdims=True)
    return rows * lax.rsqrt(mean_sq + EPS) * gain


def shards(
    resid,
    queries,
    keys,
    values,
    log_gates,
    out_gate,
    out_weight,
    post_gain,
    pre_gain,
    ffn_gain,
    gate_weight,
    up_weight,
    down_weight,
):
    rows = queries.shape[0]
    head_size = HD
    kv_local = keys.shape[1] // head_size
    q_local = queries.shape[1] // head_size
    group = q_local // kv_local
    scale = head_size ** (-0.5)
    offset = lax.axis_index("sp") * rows
    last = offset + rows - 1
    query_pos = offset + jnp.arange(rows, dtype=jnp.int32)
    key_gates = lax.all_gather(log_gates, "sp", axis=0, tiled=True)
    query_blocks = queries.reshape(rows, kv_local, group, head_size)
    query_gates = log_gates.reshape(rows, kv_local, group).transpose(1, 2, 0)

    def key_block(carry, key_rows, value_rows, start):
        count = key_rows.shape[0]

        def compute(state):
            top, denom, accum = state
            scores = (
                jnp.einsum(
                    "tkgd,skd->kgts",
                    query_blocks,
                    key_rows.reshape(count, kv_local, head_size),
                    preferred_element_type=jnp.float32,
                )
                * scale
            )
            gates_here = (
                lax.dynamic_slice_in_dim(key_gates, start, count, 0)
                .reshape(count, kv_local, group)
                .transpose(1, 2, 0)
            )
            scores = scores + query_gates[:, :, :, None] - gates_here[:, :, None, :]
            causal = (start + jnp.arange(count, dtype=jnp.int32))[None, :] <= query_pos[:, None]
            scores = jnp.where(causal[None, None], scores, -jnp.inf)
            new_top = jnp.maximum(top, jnp.max(scores, axis=-1))
            shrink = jnp.exp(top - new_top)
            weights = jnp.exp(scores - new_top[..., None])
            denom = denom * shrink + jnp.sum(weights, axis=-1)
            accum = accum * shrink[..., None] + jnp.einsum(
                "kgts,skd->kgtd",
                weights.astype(jnp.bfloat16),
                value_rows.reshape(count, kv_local, head_size),
                preferred_element_type=jnp.float32,
            )
            return (new_top, denom, accum)

        def keep(state):
            return state

        return lax.cond(start <= last, compute, keep, carry)

    start_state = (
        jnp.full((kv_local, group, rows), -1e30, jnp.float32),
        jnp.zeros((kv_local, group, rows), jnp.float32),
        jnp.zeros((kv_local, group, rows, head_size), jnp.float32),
    )
    carry = start_state
    key_rows = lax.all_gather(keys, "sp", axis=0, tiled=True)
    value_rows = lax.all_gather(values, "sp", axis=0, tiled=True)
    count = key_rows.shape[0]
    blocks = count // KEY_BLOCK
    key_split = key_rows.reshape(blocks, KEY_BLOCK, key_rows.shape[1])
    value_split = value_rows.reshape(blocks, KEY_BLOCK, value_rows.shape[1])

    def advance(state, item):
        index, key_part, value_part = item
        return (key_block(state, key_part, value_part, index * KEY_BLOCK), None)

    carry, _ = lax.scan(
        advance, carry, (jnp.arange(blocks, dtype=jnp.int32), key_split, value_split)
    )
    top, denom, accum = carry
    attended = (accum / denom[..., None]).transpose(2, 0, 1, 3).reshape(rows, q_local * head_size)
    gated = (attended * jax.nn.sigmoid(out_gate.astype(jnp.float32))).astype(jnp.bfloat16)
    projected = lax.psum_scatter(
        jnp.dot(gated, out_weight, preferred_element_type=jnp.float32).astype(jnp.bfloat16),
        "tp",
        scatter_dimension=0,
        tiled=True,
    ).astype(jnp.float32)
    mixed = resid.astype(jnp.float32) + rms_scale(projected, post_gain)
    normed = rms_scale(mixed, pre_gain).astype(jnp.bfloat16)
    normed_all = lax.all_gather(normed, "tp", axis=0, tiled=True)
    gate = jnp.dot(
        normed_all,
        lax.all_gather(gate_weight, "sp", axis=0, tiled=True),
        preferred_element_type=jnp.float32,
    )
    up = jnp.dot(
        normed_all,
        lax.all_gather(up_weight, "sp", axis=0, tiled=True),
        preferred_element_type=jnp.float32,
    )
    hidden = (jax.nn.silu(gate) * up).astype(jnp.bfloat16)
    ffn_partial = jnp.dot(
        hidden,
        lax.all_gather(down_weight, "sp", axis=1, tiled=True),
        preferred_element_type=jnp.float32,
    )
    ffn = lax.psum_scatter(
        ffn_partial.astype(jnp.bfloat16), "tp", scatter_dimension=0, tiled=True
    ).astype(jnp.float32)
    return (mixed + rms_scale(ffn, ffn_gain)).astype(jnp.bfloat16)


LANES = 128
PLANE = 4
RING = 4
MESH = pl.DeviceIdType.MESH
ANY = pl.BlockSpec(memory_space=pl.ANY)
DMA = pltpu.SemaphoreType.DMA


def pick(i, size, unit=1):
    return pl.ds(pl.multiple_of(i * size, unit), size)


def step_kernel(
    resid, queries, keys, values, slabs, out_gate, out_weight, post_gain, pre_gain, ffn_gain,
    gate_weight, up_weight, down_weight, result,
    qb, qx, kin, vin, kvp, kvb, gb, kx, vx, mb, acc, ob, att, og, ow, pb, prx, rs, mixed, gains,
    xall, gw, uw, dw, gacc, hid, om, oo, orx, osend, osum, outb,
    lsem, a_send, a_recv, z_send, z_recv, b_send, b_recv, w_send, w_recv, r_send, s_send,
    p_send, p_recv, x_send, x_recv, m_send, m_recv, o_send, o_recv, t_send, t_recv,
):
    me = lax.axis_index("sp")
    core = lax.axis_index("tp")
    p = lax.rem(me, PLANE)
    z = me // PLANE
    base = me - p
    rows, heads_w = queries.shape
    half = rows // 2
    width = resid.shape[1]
    depth = gate_weight.shape[0]
    total = rows * PLANE
    quad = heads_w // PLANE
    group = quad // HD
    hw = gw.shape[1]
    tiles = gate_weight.shape[1] // LANES
    per = hw // LANES
    f32, bf16 = jnp.float32, jnp.bfloat16

    mate = {"tp": 1 - core}
    mates = [p ^ j for j in (1, 2, 3)]
    plane_id = lambda q: {"sp": base + q}
    ring_z = lambda d: lax.rem(z + d + RING, RING)
    ring_id = lambda d: {"sp": ring_z(d) * PLANE + p}
    peers = [mate] + [plane_id(q) for q in mates] + [ring_id(d) for d in (1, 2, 3)]

    barrier = pltpu.get_barrier_semaphore()
    for peer in peers:
        pl.semaphore_signal(barrier, inc=1, device_id=peer, device_id_type=MESH)

    def remote(src, dst, send, recv, peer):
        return pltpu.make_async_remote_copy(
            src_ref=src, dst_ref=dst, send_sem=send, recv_sem=recv, device_id=peer, device_id_type=MESH)

    sent = []

    def send(*args):
        c = remote(*args)
        c.start()
        sent.append(c)

    def arrived(ref, sem):
        remote(ref, ref, sem, sem, mate).wait_recv()

    locals_ = []

    def local(src, dst):
        c = pltpu.make_async_copy(src, dst, lsem.at[len(locals_)])
        c.start()
        locals_.append(c)
        return c

    k_in = local(keys, kin)
    v_in = local(values, vin)
    cols = lambda q: pick(q, quad, LANES)
    own_rows = lambda q: pick(q, rows, 32)
    own_q = local(queries.at[:, cols(p)], qb.at[own_rows(p), :])
    own_g = local(slabs.at[p], gb.at[z, p])
    first = lambda q: jnp.minimum(q * per, tiles - per)
    wide = lambda q: pl.ds(pl.multiple_of(first(q) * LANES, LANES), hw)
    kinds = (
        (lambda q: gate_weight.at[:, wide(q)], lambda s: gw.at[pick(s, depth, LANES), :]),
        (lambda q: up_weight.at[:, wide(q)], lambda s: uw.at[pick(s, depth, LANES), :]),
        (lambda q: down_weight.at[wide(q), :], lambda s: dw.at[:, pick(s, depth, LANES)]),
    )
    own_w = [local(src(p), dst(me)) for src, dst in kinds]
    og_in = local(out_gate, og)
    ow_in = local(out_weight, ow)
    rs_in = local(resid, rs)
    gain_in = [local(g, gains.at[i]) for i, g in enumerate((post_gain, pre_gain, ffn_gain))]

    pl.semaphore_wait(barrier, len(peers))

    for i, q in enumerate(mates):
        send(slabs.at[q], gb.at[z, p], a_send.at[0, i], a_recv.at[0, p], plane_id(q))
    lane = lax.broadcasted_iota(jnp.int32, (rows, LANES), 1)
    k_in.wait()
    v_in.wait()
    for t in range(PLANE // 2):
        ts = pl.ds(t * LANES, LANES)
        kt, vt = kin[:, ts].astype(f32), vin[:, ts].astype(f32)
        kvp[2 * t] = jnp.where(lane < HD, kt, pltpu.roll(vt, HD, 1)).astype(bf16)
        kvp[2 * t + 1] = jnp.where(lane < HD, pltpu.roll(kt, HD, 1), vt).astype(bf16)
    for i, q in enumerate(mates):
        send(kvp.at[q], kvb.at[z, own_rows(p), :], a_send.at[1, i], a_recv.at[1, p], plane_id(q))
    own_kv = local(kvp.at[p], kvb.at[z, own_rows(p), :])
    for i, q in enumerate(mates):
        send(queries.at[:, cols(q)], qb.at[own_rows(p), :], a_send.at[2, i], a_recv.at[2, p], plane_id(q))

    def collect(k):
        src, dst = kinds[k]
        for i, q in enumerate(mates):
            send(src(q), dst(me), w_send.at[k, i], w_recv.at[k, me], plane_id(q))

    def ring_own(k):
        src, dst = kinds[k]
        for i, d in enumerate((1, -1)):
            send(src(p), dst(me), r_send.at[k, 0, i], w_recv.at[k, me], ring_id(d))

    def hop_one(k):
        _, dst = kinds[k]
        for j, q in enumerate(mates):
            s = base + q
            arrived(dst(s), w_recv.at[k, s])
            for i, d in enumerate((1, -1)):
                send(dst(s), dst(s), r_send.at[k, j + 1, i], w_recv.at[k, s], ring_id(d))

    def hop_two(k):
        _, dst = kinds[k]
        for q in range(PLANE):
            d = 1 if q < PLANE // 2 else -1
            s = ring_z(-d) * PLANE + q
            arrived(dst(s), w_recv.at[k, s])
            send(dst(s), dst(s), s_send.at[k, q], w_recv.at[k, s], ring_id(d))

    def all_in(k):
        _, dst = kinds[k]
        own_w[k].wait()
        for q in range(PLANE):
            d = 1 if q < PLANE // 2 else -1
            for s in (ring_z(d) * PLANE + q, ring_z(2) * PLANE + q):
                arrived(dst(s), w_recv.at[k, s])

    ring_own(0)
    collect(0)
    collect(1)
    collect(2)

    own_g.wait()
    own_kv.wait()
    for q in mates:
        arrived(gb.at[z, q], a_recv.at[0, q])
        arrived(kvb.at[z, own_rows(q), :], a_recv.at[1, q])
    up_sends = []
    for d in range(1, RING):
        peer = {"sp": me + d * PLANE}
        pair = (
            remote(gb.at[z], gb.at[z], z_send.at[0, d - 1], z_recv.at[0, d - 1], peer),
            remote(kvb.at[z], kvb.at[z], z_send.at[1, d - 1], z_recv.at[1, d - 1], peer),
        )
        up_sends.append((d, pair))

        @pl.when(z + d < RING)
        def _(pair=pair):
            for c in pair:
                c.start()

    ring_own(1)
    ring_own(2)

    def build(s):
        kv = kvb[s].astype(f32)
        g = []
        for t in range(total // LANES):
            g.append(None)
        for q in range(PLANE):
            tile0 = (rows * q) // LANES
            for j in range(gb.shape[3] // LANES):
                part = gb[s, q, :, j * LANES:(j + 1) * LANES]
                if tile0 + j < len(g):
                    g[tile0 + j] = part if g[tile0 + j] is None else g[tile0 + j] + part
        neg = -jnp.concatenate(g, axis=1)
        hi = neg.astype(bf16).astype(f32)
        rest = neg - hi
        mid = rest.astype(bf16).astype(f32)
        low = rest - mid
        pad = jnp.zeros((LANES - HD - 24, total), f32)
        kx[...] = jnp.concatenate([kv.T[:HD], hi, mid, low, pad], axis=0).astype(bf16)
        lk = lax.broadcasted_iota(jnp.int32, (total, LANES), 1)
        vx[...] = jnp.where(lk < HD, 1.0, kv).astype(bf16)

    build(z)
    own_q.wait()
    for q in mates:
        arrived(qb.at[own_rows(q), :], a_recv.at[2, q])
    lq = lax.broadcasted_iota(jnp.int32, (total, LANES), 1)
    for j in range(group):
        t = qb[:, (j // 2) * LANES:(j // 2 + 1) * LANES].astype(f32) * (HD ** -0.5)
        if j % 2:
            t = pltpu.roll(t, HD, 1)
        hot = (lq == HD + j) | (lq == HD + 8 + j) | (lq == HD + 16 + j)
        qx[j * total:(j + 1) * total, :] = jnp.where(lq < HD, t, jnp.where(hot, 1.0, 0.0)).astype(bf16)

    blk = total // 3
    for i in range(3):
        nk = (i + 1) * blk

        def diagonal(h, _, i=i, nk=nk):
            rs_ = pl.ds(pl.multiple_of(h * total + i * blk, blk), blk)
            s = jnp.dot(qx[rs_, :], kx[:, :nk], preferred_element_type=f32)
            r = lax.broadcasted_iota(jnp.int32, s.shape, 0) + i * blk
            c = lax.broadcasted_iota(jnp.int32, s.shape, 1)
            s = jnp.where(c <= r, s, -1e30)
            m = jnp.max(s, axis=1, keepdims=True)
            w = jnp.exp(s - m).astype(bf16)
            mb[rs_, :] = m
            acc[rs_, :] = jnp.dot(w, vx[:nk, :], preferred_element_type=f32)
            return 0

        lax.fori_loop(0, group, diagonal, 0)

    hop_one(0)

    def full(b, _):
        rs_ = pl.ds(pl.multiple_of(b * blk, blk), blk)
        s = jnp.dot(qx[rs_, :], kx[...], preferred_element_type=f32)
        old = mb[rs_, :]
        m = jnp.maximum(old, jnp.max(s, axis=1, keepdims=True))
        w = jnp.exp(s - m).astype(bf16)
        mb[rs_, :] = m
        acc[rs_, :] = acc[rs_, :] * jnp.exp(old - m) + jnp.dot(w, vx[...], preferred_element_type=f32)
        return 0

    def plane_step(d):
        @pl.when(z >= d)
        def _():
            s = z - d
            arrived(gb.at[s], z_recv.at[0, d - 1])
            arrived(kvb.at[s], z_recv.at[1, d - 1])
            build(s)
            lax.fori_loop(0, 3 * group, full, 0)

    plane_step(1)
    hop_one(1)
    plane_step(2)
    hop_one(2)
    plane_step(3)

    lane_b = lax.broadcasted_iota(jnp.int32, (blk, LANES), 1)
    for t in range(group // 2):
        def finish(i, _, t=t):
            even = acc[pl.ds(pl.multiple_of(2 * t * total + i * blk, blk), blk), :]
            odd = acc[pl.ds(pl.multiple_of((2 * t + 1) * total + i * blk, blk), blk), :]
            even = even / even[:, :1]
            odd = odd / odd[:, :1]
            both = jnp.where(lane_b < HD, pltpu.roll(even, HD, 1), odd)
            ob[pl.ds(pl.multiple_of(i * blk, blk), blk), t * LANES:(t + 1) * LANES] = both.astype(bf16)
            return 0

        lax.fori_loop(0, 3, finish, 0)

    for i, q in enumerate(mates):
        send(ob.at[own_rows(q), :], att.at[:, cols(p)], b_send.at[i], b_recv.at[p], plane_id(q))
    own_att = local(ob.at[own_rows(p), :], att.at[:, cols(p)])
    hop_two(0)
    og_in.wait()
    ow_in.wait()
    rs_in.wait()
    for c in gain_in:
        c.wait()
    own_att.wait()
    for q in mates:
        arrived(att.at[:, cols(q)], b_recv.at[q])
    gated = (att[...].astype(f32) * jax.nn.sigmoid(og[...].astype(f32))).astype(bf16)
    att[...] = gated
    wn = 512

    def project(n, _):
        cs = pick(n, wn, LANES)
        part = jnp.dot(att[...], ow[:, cs], preferred_element_type=f32).astype(bf16)
        pb[0, :, cs] = part[:half]
        pb[1, :, cs] = part[half:]
        return 0

    lax.fori_loop(0, width // wn, project, 0)
    send(pb.at[1 - core], prx, p_send, p_recv, mate)
    hop_two(1)
    arrived(prx, p_recv)

    def scale(v, gain):
        return v * lax.rsqrt(jnp.mean(v * v, axis=-1, keepdims=True) + EPS) * gain

    projected = pb[core].astype(f32) + prx[...].astype(f32)
    mix = rs[...].astype(f32) + scale(projected, gains[0])
    mixed[...] = mix
    slot = lambda q, c: pl.ds(pl.multiple_of(q * rows + c * half, 32), half)
    xall[slot(p, core), :] = scale(mix, gains[1]).astype(bf16)
    mine = xall.at[slot(p, core), :]
    for i, q in enumerate(mates):
        send(mine, mine, x_send.at[i], x_recv.at[p], plane_id(q))
    send(mine, mine, m_send.at[0], m_recv.at[p], mate)
    hop_two(2)
    for i, q in enumerate(mates):
        there = xall.at[slot(q, core), :]
        arrived(there, x_recv.at[q])
        send(there, there, m_send.at[i + 1], m_recv.at[q], mate)
    for q in (p, *mates):
        arrived(xall.at[slot(q, 1 - core), :], m_recv.at[q])

    hn = 256
    all_in(0)

    def gate_step(n, _):
        cs = pick(n, hn, LANES)
        gacc[:, cs] = jnp.dot(xall[...], gw[:, cs], preferred_element_type=f32)
        return 0

    lax.fori_loop(0, hw // hn, gate_step, 0)
    all_in(1)
    dup = p * per - first(p)

    def up_step(n, _):
        cs = pick(n, hn, LANES)
        up = jnp.dot(xall[...], uw[:, cs], preferred_element_type=f32)
        g = gacc[:, cs]
        h = g / (1.0 + jnp.exp(-g)) * up
        unit = lax.broadcasted_iota(jnp.int32, h.shape, 1) + n * hn
        hid[:, cs] = jnp.where(unit >= dup * LANES, h, 0.0).astype(bf16)
        return 0

    lax.fori_loop(0, hw // hn, up_step, 0)
    all_in(2)

    order = [p ^ 3, p ^ 1, p ^ 2, p]
    for i, q in enumerate(order):
        def down_step(n, _, i=i, q=q):
            cs = pick(n, wn, LANES)
            part = jnp.dot(hid[own_rows(q), :], dw[:, cs], preferred_element_type=f32)
            low_, high = part[:half], part[half:]
            om[i, :, cs] = jnp.where(core == 0, low_, high)
            oo[i, :, cs] = jnp.where(core == 0, high, low_).astype(bf16)
            return 0

        lax.fori_loop(0, width // wn, down_step, 0)
        send(oo.at[i], orx.at[i], t_send.at[i], t_recv.at[i], mate)
        if i:
            finish_out(i - 1, order, arrived, send, orx, om, osend, osum, t_recv, o_send, o_recv, p, plane_id)
    arrived(orx.at[3], t_recv.at[3])
    ffn = om[3] + orx[3].astype(f32)
    for q in mates:
        arrived(osum.at[q], o_recv.at[q])
        ffn += osum[q].astype(f32)
    outb[...] = (mixed[...] + scale(ffn, gains[2])).astype(bf16)
    last = local(outb, result)
    for c in sent:
        c.wait_send()
    for d, pair in up_sends:
        @pl.when(z + d < RING)
        def _(pair=pair):
            for c in pair:
                c.wait_send()
    last.wait()


def finish_out(i, order, arrived, send, orx, om, osend, osum, t_recv, o_send, o_recv, p, plane_id):
    arrived(orx.at[i], t_recv.at[i])
    osend[i] = (om[i] + orx[i].astype(jnp.float32)).astype(jnp.bfloat16)
    send(osend.at[i], osum.at[p], o_send.at[i], o_recv.at[p], plane_id(order[i]))


def fast_shards(n, resid, queries, keys, values, log_gates, out_gate, out_weight, post_gain,
                pre_gain, ffn_gain, gate_weight, up_weight, down_weight):
    rows, heads_w = queries.shape
    width = resid.shape[1]
    total = rows * PLANE
    heads = heads_w // HD
    group = heads // PLANE
    half = rows // 2
    tiles = gate_weight.shape[1] // LANES
    hw = -(-tiles // PLANE) * LANES
    slab_w = -(-(rows + HD) // LANES) * LANES
    odd = lax.rem(lax.axis_index("sp"), 2) == 1
    slabs = log_gates.T.reshape(PLANE, group, rows)
    fill = lambda left: jnp.pad(slabs, ((0, 0), (0, 8 - group), (left, slab_w - rows - left)))
    slabs = jnp.where(odd, fill(HD), fill(0))
    bf16, f32 = jnp.bfloat16, jnp.float32
    vm = pltpu.VMEM
    gain = lambda g: g.reshape(1, width)
    return pl.pallas_call(
        step_kernel,
        out_shape=jax.ShapeDtypeStruct(resid.shape, resid.dtype),
        in_specs=[ANY] * 13,
        out_specs=ANY,
        scratch_shapes=[
            vm((total, heads_w // PLANE), bf16),
            vm((group * total, LANES), bf16),
            vm(keys.shape, bf16), vm(values.shape, bf16),
            vm((PLANE, rows, LANES), bf16),
            vm((RING, total, LANES), bf16),
            vm((RING, PLANE, 8, slab_w), f32),
            vm((LANES, total), bf16), vm((total, LANES), bf16),
            vm((group * total, 1), f32), vm((group * total, LANES), f32),
            vm((total, heads_w // PLANE), bf16),
            vm((rows, heads_w), bf16), vm((rows, heads_w), bf16),
            vm(out_weight.shape, bf16),
            vm((2, half, width), bf16), vm((half, width), bf16), vm((half, width), bf16),
            vm((half, width), f32), vm((3, 1, width), f32),
            vm((total, width), bf16),
            vm((width, hw), bf16), vm((width, hw), bf16), vm((hw, width), bf16),
            vm((total, hw), f32), vm((total, hw), bf16),
            vm((4, half, width), f32), vm((4, half, width), bf16), vm((4, half, width), bf16),
            vm((3, half, width), bf16), vm((PLANE, half, width), bf16), vm((half, width), bf16),
            DMA((16,)), DMA((3, 3)), DMA((3, PLANE)), DMA((2, 3)), DMA((2, 3)),
            DMA((3,)), DMA((PLANE,)), DMA((3, 3)), DMA((3, n)), DMA((3, PLANE, 2)), DMA((3, PLANE)),
            DMA, DMA, DMA((3,)), DMA((PLANE,)), DMA((PLANE,)), DMA((PLANE,)),
            DMA((3,)), DMA((PLANE,)), DMA((4,)), DMA((4,)),
        ],
        compiler_params=pltpu.CompilerParams(
            collective_id=1, has_side_effects=True, vmem_limit_bytes=62 * 1024 * 1024),
    )(resid, queries, keys, values, slabs, out_gate, out_weight, gain(post_gain), gain(pre_gain),
      gain(ffn_gain), gate_weight, up_weight, down_weight)


def solution(mesh):
    n, cores = mesh.shape["sp"], mesh.shape["tp"]

    def body(*args):
        queries, keys, gate_weight = args[1], args[2], args[10]
        fits = cores == 2 and n == PLANE * RING and keys.shape[1] == PLANE * HD
        fits = fits and queries.shape[1] == 4 * keys.shape[1] and queries.shape[0] % 64 == 0
        fits = fits and gate_weight.shape[1] % LANES == 0 and gate_weight.shape[0] % LANES == 0
        return fast_shards(n, *args) if fits else shards(*args)

    in_specs = (
        P(("sp", "tp"), None),
        P("sp", "tp"),
        P("sp", "tp"),
        P("sp", "tp"),
        P("sp", "tp"),
        P("sp", "tp"),
        P("tp", None),
        P(),
        P(),
        P(),
        P("sp", "tp"),
        P("sp", "tp"),
        P("tp", "sp"),
    )
    out_specs = P(("sp", "tp"), None)
    return jax.shard_map(body, mesh=mesh, in_specs=in_specs, out_specs=out_specs, check_vma=False)
```

```python
import functools

import jax
import jax.numpy as jnp
from jax import lax
from jax.experimental import pallas as pl
from jax.experimental.pallas import tpu as pltpu
from jax.sharding import PartitionSpec as P

HD = 64


EPS = 1e-06
KEY_BLOCK = 512


def rms_scale(rows, gain):
    mean_sq = jnp.mean(rows * rows, axis=-1, keepdims=True)
    return rows * lax.rsqrt(mean_sq + EPS) * gain


def shards(
    resid,
    queries,
    keys,
    values,
    log_gates,
    out_gate,
    out_weight,
    post_gain,
    pre_gain,
    ffn_gain,
    gate_weight,
    up_weight,
    down_weight,
):
    rows = queries.shape[0]
    head_size = HD
    kv_local = keys.shape[1] // head_size
    q_local = queries.shape[1] // head_size
    group = q_local // kv_local
    scale = head_size ** (-0.5)
    offset = lax.axis_index("sp") * rows
    last = offset + rows - 1
    query_pos = offset + jnp.arange(rows, dtype=jnp.int32)
    key_gates = lax.all_gather(log_gates, "sp", axis=0, tiled=True)
    query_blocks = queries.reshape(rows, kv_local, group, head_size)
    query_gates = log_gates.reshape(rows, kv_local, group).transpose(1, 2, 0)

    def key_block(carry, key_rows, value_rows, start):
        count = key_rows.shape[0]

        def compute(state):
            top, denom, accum = state
            scores = (
                jnp.einsum(
                    "tkgd,skd->kgts",
                    query_blocks,
                    key_rows.reshape(count, kv_local, head_size),
                    preferred_element_type=jnp.float32,
                )
                * scale
            )
            gates_here = (
                lax.dynamic_slice_in_dim(key_gates, start, count, 0)
                .reshape(count, kv_local, group)
                .transpose(1, 2, 0)
            )
            scores = scores + query_gates[:, :, :, None] - gates_here[:, :, None, :]
            causal = (start + jnp.arange(count, dtype=jnp.int32))[None, :] <= query_pos[:, None]
            scores = jnp.where(causal[None, None], scores, -jnp.inf)
            new_top = jnp.maximum(top, jnp.max(scores, axis=-1))
            shrink = jnp.exp(top - new_top)
            weights = jnp.exp(scores - new_top[..., None])
            denom = denom * shrink + jnp.sum(weights, axis=-1)
            accum = accum * shrink[..., None] + jnp.einsum(
                "kgts,skd->kgtd",
                weights.astype(jnp.bfloat16),
                value_rows.reshape(count, kv_local, head_size),
                preferred_element_type=jnp.float32,
            )
            return (new_top, denom, accum)

        def keep(state):
            return state

        return lax.cond(start <= last, compute, keep, carry)

    start_state = (
        jnp.full((kv_local, group, rows), -1e30, jnp.float32),
        jnp.zeros((kv_local, group, rows), jnp.float32),
        jnp.zeros((kv_local, group, rows, head_size), jnp.float32),
    )
    carry = start_state
    key_rows = lax.all_gather(keys, "sp", axis=0, tiled=True)
    value_rows = lax.all_gather(values, "sp", axis=0, tiled=True)
    count = key_rows.shape[0]
    blocks = count // KEY_BLOCK
    key_split = key_rows.reshape(blocks, KEY_BLOCK, key_rows.shape[1])
    value_split = value_rows.reshape(blocks, KEY_BLOCK, value_rows.shape[1])

    def advance(state, item):
        index, key_part, value_part = item
        return (key_block(state, key_part, value_part, index * KEY_BLOCK), None)

    carry, _ = lax.scan(
        advance, carry, (jnp.arange(blocks, dtype=jnp.int32), key_split, value_split)
    )
    top, denom, accum = carry
    attended = (accum / denom[..., None]).transpose(2, 0, 1, 3).reshape(rows, q_local * head_size)
    gated = (attended * jax.nn.sigmoid(out_gate.astype(jnp.float32))).astype(jnp.bfloat16)
    projected = lax.psum_scatter(
        jnp.dot(gated, out_weight, preferred_element_type=jnp.float32).astype(jnp.bfloat16),
        "tp",
        scatter_dimension=0,
        tiled=True,
    ).astype(jnp.float32)
    mixed = resid.astype(jnp.float32) + rms_scale(projected, post_gain)
    normed = rms_scale(mixed, pre_gain).astype(jnp.bfloat16)
    normed_all = lax.all_gather(normed, "tp", axis=0, tiled=True)
    gate = jnp.dot(
        normed_all,
        lax.all_gather(gate_weight, "sp", axis=0, tiled=True),
        preferred_element_type=jnp.float32,
    )
    up = jnp.dot(
        normed_all,
        lax.all_gather(up_weight, "sp", axis=0, tiled=True),
        preferred_element_type=jnp.float32,
    )
    hidden = (jax.nn.silu(gate) * up).astype(jnp.bfloat16)
    ffn_partial = jnp.dot(
        hidden,
        lax.all_gather(down_weight, "sp", axis=1, tiled=True),
        preferred_element_type=jnp.float32,
    )
    ffn = lax.psum_scatter(
        ffn_partial.astype(jnp.bfloat16), "tp", scatter_dimension=0, tiled=True
    ).astype(jnp.float32)
    return (mixed + rms_scale(ffn, ffn_gain)).astype(jnp.bfloat16)


LANES = 128
PLANE = 4
RING = 4
MESH = pl.DeviceIdType.MESH
ANY = pl.BlockSpec(memory_space=pl.ANY)
DMA = pltpu.SemaphoreType.DMA


def pick(i, size, unit=1):
    return pl.ds(pl.multiple_of(i * size, unit), size)


def step_kernel(
    resid, queries, keys, values, slabs, out_gate, out_weight, post_gain, pre_gain, ffn_gain,
    gate_weight, up_weight, down_weight, result,
    qb, qx, kin, vin, kvp, kvb, gb, kx, vx, mb, acc, ob, att, og, ow, pb, prx, rs, mixed, gains,
    xall, gw, uw, dw, gacc, hid, om, oo, orx, osend, ubuf, dbuf, outb,
    lsem, a_send, a_recv, z_send, z_recv, b_send, b_recv, w_send, w_recv, r_send, s_send, own_sem,
    p_send, p_recv, x_send, x_recv, m_send, m_recv, o_send, u_recv, d_recv, t_send, t_recv,
):
    me = lax.axis_index("sp")
    core = lax.axis_index("tp")
    p = lax.rem(me, PLANE)
    z = me // PLANE
    base = me - p
    rows, heads_w = queries.shape
    half = rows // 2
    width = resid.shape[1]
    depth = gate_weight.shape[0]
    total = rows * PLANE
    quad = heads_w // PLANE
    group = quad // HD
    hw = gw.shape[1]
    tiles = gate_weight.shape[1] // LANES
    width_of = [(tiles // RING + (c < tiles % RING)) * LANES for c in range(RING)]
    start_of = [sum(width_of[:c]) for c in range(RING)]
    f32, bf16 = jnp.float32, jnp.bfloat16

    mate = {"tp": 1 - core}
    mates = [p ^ j for j in (1, 2, 3)]
    lines = [z ^ j for j in (1, 2, 3)]
    plane_id = lambda q: {"sp": base + q}
    line_id = lambda c: {"sp": c * PLANE + p}
    peers = [mate] + [plane_id(q) for q in mates] + [line_id(c) for c in lines]
    barrier = pltpu.get_barrier_semaphore()
    for peer in peers:
        pl.semaphore_signal(barrier, inc=1, device_id=peer, device_id_type=MESH)

    def remote(src, dst, send, recv, peer):
        return pltpu.make_async_remote_copy(
            src_ref=src, dst_ref=dst, send_sem=send, recv_sem=recv, device_id=peer, device_id_type=MESH)

    sent = []

    def send(*args, when=None):
        c = remote(*args)
        sent.append((when, c))
        if when is None:
            c.start()
        else:
            pl.when(when)(c.start)

    def arrived(ref, sem):
        remote(ref, ref, sem, sem, mate).wait_recv()

    locals_ = []

    def local(src, dst):
        c = pltpu.make_async_copy(src, dst, lsem.at[len(locals_)])
        c.start()
        locals_.append(c)
        return c

    if tiles % RING:
        @pl.when(z >= tiles % RING)
        def _():
            gw[:, width_of[-1]:] = jnp.zeros((width, hw - width_of[-1]), bf16)
            uw[:, width_of[-1]:] = jnp.zeros((width, hw - width_of[-1]), bf16)
            dw[width_of[-1]:, :] = jnp.zeros((hw - width_of[-1], width), bf16)

    k_in = local(keys, kin)
    v_in = local(values, vin)
    cols = lambda q: pick(q, quad, LANES)
    own_rows = lambda q: pick(q, rows, 32)
    own_q = local(queries.at[:, cols(p)], qb.at[own_rows(p), :])
    own_g = local(slabs.at[p], gb.at[z, p])
    wide = lambda c: pl.ds(start_of[c], width_of[c])
    kinds = (
        (lambda c: gate_weight.at[:, wide(c)], lambda s, c: gw.at[pick(s, depth, LANES), :width_of[c]]),
        (lambda c: up_weight.at[:, wide(c)], lambda s, c: uw.at[pick(s, depth, LANES), :width_of[c]]),
        (lambda c: down_weight.at[wide(c), :], lambda s, c: dw.at[:width_of[c], pick(s, depth, LANES)]),
    )
    og_in = local(out_gate, og)
    ow_in = local(out_weight, ow)
    rs_in = local(resid, rs)
    gain_in = [local(g, gains.at[i]) for i, g in enumerate((post_gain, pre_gain, ffn_gain))]
    pl.semaphore_wait(barrier, len(peers))
    for i, q in enumerate(mates):
        send(slabs.at[q], gb.at[z, p], a_send.at[0, i], a_recv.at[0, p], plane_id(q))
    lane = lax.broadcasted_iota(jnp.int32, (rows, LANES), 1)
    k_in.wait()
    v_in.wait()
    for t in range(PLANE // 2):
        ts = pl.ds(t * LANES, LANES)
        kt, vt = kin[:, ts].astype(f32), vin[:, ts].astype(f32)
        kvp[2 * t] = jnp.where(lane < HD, kt, pltpu.roll(vt, HD, 1)).astype(bf16)
        kvp[2 * t + 1] = jnp.where(lane < HD, pltpu.roll(kt, HD, 1), vt).astype(bf16)
    for i, q in enumerate(mates):
        send(kvp.at[q], kvb.at[z, own_rows(p), :], a_send.at[1, i], a_recv.at[1, p], plane_id(q))
    own_kv = local(kvp.at[p], kvb.at[z, own_rows(p), :])
    for i, q in enumerate(mates):
        send(queries.at[:, cols(q)], qb.at[own_rows(p), :], a_send.at[2, i], a_recv.at[2, p], plane_id(q))

    sides = (p ^ 1, p ^ 2)
    posted = [[] for _ in range(RING)]

    def post(zv, make):
        make().start()
        posted[zv].append(make)

    def own(zv, k):
        src, dst = kinds[k]
        pltpu.make_async_copy(src(zv), dst(me, zv), own_sem.at[k]).start()
        for i in range(2):
            post(zv, lambda i=i: remote(
                src(zv), dst(me, zv), r_send.at[k, 0, i], w_recv.at[k, me], plane_id(sides[i])))

    def along(zv, k, c):
        src, dst = kinds[k]
        post(zv, lambda: remote(src(c), dst(me, c), w_send.at[k, c], w_recv.at[k, me], line_id(c)))

    def hop(zv, k, c):
        _, dst = kinds[k]
        there = lambda: dst(c * PLANE + p, zv)
        arrived(there(), w_recv.at[k, c * PLANE + p])
        for i in range(2):
            post(zv, lambda i=i: remote(
                there(), there(), r_send.at[k, 1 + c, i], w_recv.at[k, c * PLANE + p], plane_id(sides[i])))

    def turn(zv, k):
        _, dst = kinds[k]
        for c in range(RING):
            i = 0 if c < RING // 2 else 1
            there = lambda c=c, i=i: dst(c * PLANE + sides[i], zv)
            arrived(there(), w_recv.at[k, c * PLANE + sides[i]])
            post(zv, lambda c=c, i=i, there=there: remote(
                there(), there(), s_send.at[k, c], w_recv.at[k, c * PLANE + sides[i]], plane_id(sides[1 - i])))

    def all_in(k):
        src, dst = kinds[k]
        for zv in range(RING):
            @pl.when(z == zv)
            def _(zv=zv):
                pltpu.make_async_copy(src(zv), dst(me, zv), own_sem.at[k]).wait()
                for c in range(RING):
                    i = 0 if c < RING // 2 else 1
                    for s in (c * PLANE + sides[1 - i], c * PLANE + (p ^ 3)):
                        arrived(dst(s, zv), w_recv.at[k, s])

    def stage(*table):
        for zv, ops in enumerate(table):
            if ops:
                @pl.when(z == zv)
                def _(zv=zv, ops=ops):
                    for f, *args in ops:
                        f(zv, *args)

    downs = lambda zv: [(along, k, c) for k in range(3) for c in range(zv - 1, -1, -1)]
    stage(*[[(own, 0), (own, 1), (own, 2)] + downs(zv) for zv in range(RING)])
    own_g.wait()
    own_kv.wait()
    for q in mates:
        arrived(gb.at[z, q], a_recv.at[0, q])
        arrived(kvb.at[z, own_rows(q), :], a_recv.at[1, q])

    def upward(s, d):
        peer = line_id(jnp.minimum(z + 1, RING - 1))
        ok = (z < RING - 1) & (s >= 0)
        s = jnp.maximum(s, 0)
        send(gb.at[s], gb.at[s], z_send.at[0, d], z_recv.at[0, s], peer, when=ok)
        send(kvb.at[s], kvb.at[s], z_send.at[1, d], z_recv.at[1, s], peer, when=ok)

    upward(z, 0)
    stage([(along, 0, 1), (along, 1, 1), (along, 2, 1)], [(along, 0, 2)], [(along, 0, 3)], [])
    def build(s):
        kv = kvb[s].astype(f32)
        g = []
        for t in range(total // LANES):
            g.append(None)
        for q in range(PLANE):
            tile0 = (rows * q) // LANES
            for j in range(gb.shape[3] // LANES):
                part = gb[s, q, :, j * LANES:(j + 1) * LANES]
                if tile0 + j < len(g):
                    g[tile0 + j] = part if g[tile0 + j] is None else g[tile0 + j] + part
        neg = -jnp.concatenate(g, axis=1)
        hi = neg.astype(bf16).astype(f32)
        rest = neg - hi
        mid = rest.astype(bf16).astype(f32)
        low = rest - mid
        pad = jnp.zeros((LANES - HD - 24, total), f32)
        kx[...] = jnp.concatenate([kv.T[:HD], hi, mid, low, pad], axis=0).astype(bf16)
        lk = lax.broadcasted_iota(jnp.int32, (total, LANES), 1)
        vx[...] = jnp.where(lk < HD, 1.0, kv).astype(bf16)
    build(z)
    own_q.wait()
    for q in mates:
        arrived(qb.at[own_rows(q), :], a_recv.at[2, q])
    lq = lax.broadcasted_iota(jnp.int32, (total, LANES), 1)
    for j in range(group):
        t = qb[:, (j // 2) * LANES:(j // 2 + 1) * LANES].astype(f32) * (HD ** -0.5)
        if j % 2:
            t = pltpu.roll(t, HD, 1)
        hot = (lq == HD + j) | (lq == HD + 8 + j) | (lq == HD + 16 + j)
        qx[j * total:(j + 1) * total, :] = jnp.where(lq < HD, t, jnp.where(hot, 1.0, 0.0)).astype(bf16)
    blk = total // 3
    for i in range(3):
        nk = (i + 1) * blk

        def diagonal(h, _, i=i, nk=nk):
            at = [pl.ds(pl.multiple_of((2 * h + e) * total + i * blk, blk), blk) for e in range(2)]
            s = [jnp.dot(qx[r, :], kx[:, :nk], preferred_element_type=f32) for r in at]
            r = lax.broadcasted_iota(jnp.int32, s[0].shape, 0) + i * blk
            c = lax.broadcasted_iota(jnp.int32, s[0].shape, 1)
            s = [jnp.where(c <= r, t, -1e30) for t in s]
            m = [jnp.max(t, axis=1, keepdims=True) for t in s]
            w = [jnp.exp(t - u).astype(bf16) for t, u in zip(s, m)]
            for e, r in enumerate(at):
                mb[r, :] = m[e]
                acc[r, :] = jnp.dot(w[e], vx[:nk, :], preferred_element_type=f32)
            return 0

        lax.fori_loop(0, group // 2, diagonal, 0)

    def full(b, _):
        at = [pl.ds(pl.multiple_of((4 * b + e) * blk, blk), blk) for e in range(4)]
        s = [jnp.dot(qx[r, :], kx[...], preferred_element_type=f32) for r in at]
        old = [mb[r, :] for r in at]
        m = [jnp.maximum(o, jnp.max(t, axis=1, keepdims=True)) for o, t in zip(old, s)]
        w = [jnp.exp(t - u).astype(bf16) for t, u in zip(s, m)]
        for e, r in enumerate(at):
            mb[r, :] = m[e]
            more = jnp.dot(w[e], vx[...], preferred_element_type=f32)
            acc[r, :] = acc[r, :] * jnp.exp(old[e] - m[e]) + more
        return 0

    def plane_step(d, *table):
        @pl.when(z >= d)
        def _():
            arrived(gb.at[z - d], z_recv.at[0, z - d])
            arrived(kvb.at[z - d], z_recv.at[1, z - d])

        if d < RING - 1:
            upward(z - d, d)
        stage(*table)

        @pl.when(z >= d)
        def _():
            build(z - d)
            lax.fori_loop(0, 3 * group // 4, full, 0)
    plane_step(1, [], [(along, 0, 3)], [(hop, 0, 3)], [])
    plane_step(2, [], [(along, 1, 2), (along, 2, 2), (along, 1, 3), (along, 2, 3)],
               [(hop, 1, 3), (along, 1, 3), (along, 2, 3)], [])
    plane_step(3, [], [], [], [(hop, 0, 2)])
    lane_b = lax.broadcasted_iota(jnp.int32, (blk, LANES), 1)
    for t in range(group // 2):
        def finish(i, _, t=t):
            even = acc[pl.ds(pl.multiple_of(2 * t * total + i * blk, blk), blk), :]
            odd = acc[pl.ds(pl.multiple_of((2 * t + 1) * total + i * blk, blk), blk), :]
            even = even / even[:, :1]
            odd = odd / odd[:, :1]
            both = jnp.where(lane_b < HD, pltpu.roll(even, HD, 1), odd)
            ob[pl.ds(pl.multiple_of(i * blk, blk), blk), t * LANES:(t + 1) * LANES] = both.astype(bf16)
            return 0

        lax.fori_loop(0, 3, finish, 0)
    for i, q in enumerate(mates):
        send(ob.at[own_rows(q), :], att.at[:, cols(p)], b_send.at[i], b_recv.at[p], plane_id(q))
    own_att = local(ob.at[own_rows(p), :], att.at[:, cols(p)])
    stage([(along, k, c) for k in range(3) for c in (2, 3)] + [(hop, 0, 1), (hop, 0, 3), (hop, 0, 2)],
          [(hop, 0, 2), (hop, 0, 3), (hop, 0, 0)], [(hop, 2, 3), (hop, 0, 1)], [(hop, 0, 1)])
    og_in.wait()
    ow_in.wait()
    rs_in.wait()
    for c in gain_in:
        c.wait()
    own_att.wait()
    for q in mates:
        arrived(att.at[:, cols(q)], b_recv.at[q])
    gated = (att[...].astype(f32) * jax.nn.sigmoid(og[...].astype(f32))).astype(bf16)
    att[...] = gated
    wn = 512

    def project(n, _):
        cs = pick(n, wn, LANES)
        part = jnp.dot(att[...], ow[:, cs], preferred_element_type=f32).astype(bf16)
        pb[0, :, cs] = part[:half]
        pb[1, :, cs] = part[half:]
        return 0

    lax.fori_loop(0, width // wn, project, 0)
    send(pb.at[1 - core], prx, p_send, p_recv, mate)
    arrived(prx, p_recv)

    def scale(v, gain):
        return v * lax.rsqrt(jnp.mean(v * v, axis=-1, keepdims=True) + EPS) * gain

    projected = pb[core].astype(f32) + prx[...].astype(f32)
    mix = rs[...].astype(f32) + scale(projected, gains[0])
    mixed[...] = mix
    slot = lambda c, h: xall.at[pl.ds(pl.multiple_of(c * rows + h * half, 32), half), :]
    mine = slot(z, core)
    mine[...] = scale(mix, gains[1]).astype(bf16)
    above = line_id(jnp.minimum(z + 1, RING - 1))
    below = line_id(jnp.maximum(z - 1, 0))
    send(mine, mine, x_send.at[0], x_recv.at[z], above, when=z < RING - 1)
    send(mine, mine, x_send.at[1], x_recv.at[z], below, when=z > 0)
    send(mine, mine, m_send.at[0], m_recv.at[z], mate)
    def rows_from(zv, c):
        there = lambda: slot(c, core)
        arrived(there(), x_recv.at[c])
        nxt = zv + 1 if c < zv else zv - 1
        if 0 <= nxt < RING:
            post(zv, lambda: remote(there(), there(), x_send.at[2 + c], x_recv.at[c], line_id(nxt)))
        post(zv, lambda: remote(there(), there(), m_send.at[c + 1], m_recv.at[c], mate))

    stage(
        [(hop, 1, 1), (hop, 1, 3), (hop, 1, 2), (turn, 0), (hop, 2, 1), (hop, 2, 3), (hop, 2, 2), (turn, 1)],
        [(hop, 1, 2), (hop, 1, 0), (hop, 1, 3), (turn, 0), (hop, 2, 0), (hop, 2, 2), (hop, 2, 3), (turn, 1)],
        [(hop, 0, 0), (hop, 1, 1), (turn, 0), (rows_from, 3), (hop, 1, 0), (hop, 2, 1), (turn, 1), (hop, 2, 0)],
        [(hop, 0, 0), (hop, 1, 2), (turn, 0), (hop, 1, 1), (hop, 1, 0), (hop, 2, 2), (turn, 1), (hop, 2, 1),
         (hop, 2, 0)],
    )
    stage(
        [(turn, 2), (rows_from, 1), (rows_from, 2), (rows_from, 3)],
        [(rows_from, 0), (rows_from, 2), (rows_from, 3), (turn, 2)],
        [(rows_from, 1), (rows_from, 0), (turn, 2)],
        [(turn, 2), (rows_from, 2), (rows_from, 1), (rows_from, 0)],
    )
    for c in range(RING):
        arrived(slot(c, 1 - core), m_recv.at[c])

    hn = 256
    all_in(0)
    def gate_step(n, _):
        cs = pick(n, hn, LANES)
        gacc[:, cs] = jnp.dot(xall[...], gw[:, cs], preferred_element_type=f32)
        return 0

    lax.fori_loop(0, hw // hn, gate_step, 0)
    all_in(1)
    valid = jnp.where(z < tiles % RING, hw, width_of[-1])

    def up_step(n, _):
        cs = pick(n, hn, LANES)
        up = jnp.dot(xall[...], uw[:, cs], preferred_element_type=f32)
        g = gacc[:, cs]
        h = g / (1.0 + jnp.exp(-g)) * up
        unit = lax.broadcasted_iota(jnp.int32, h.shape, 1) + n * hn
        hid[:, cs] = jnp.where(unit < valid, h, 0.0).astype(bf16)
        return 0

    lax.fori_loop(0, hw // hn, up_step, 0)
    all_in(2)
    edge = (z == 0) | (z == RING - 1)

    parts = 2
    strip = lambda h: pl.ds(h * (width // parts), width // parts)

    def onward(r, h, when):
        osend[r, :, strip(h)] = om[r, :, strip(h)].astype(bf16)
        peer = line_id(jnp.clip(jnp.where(r > z, z + 1, z - 1), 0, RING - 1))
        for buf, sem, ok in ((ubuf, u_recv, r > z), (dbuf, d_recv, r < z)):
            src = osend.at[r, :, strip(h)]
            c = remote(src, buf.at[r, :, strip(h)], o_send.at[r, h], sem.at[r, h], peer)
            pl.when(when & ok)(c.start)

    def merge(r, h):
        arrived(orx.at[r, :, strip(h)], t_recv.at[r, h])
        om[r, :, strip(h)] = om[r, :, strip(h)] + orx[r, :, strip(h)].astype(f32)

    order = [(z ^ j, h) for j in (3, 2, 1, 0) for h in range(parts)]

    def pass_on(q, h):
        merge(q, h)
        pl.when(edge & (q != z))(functools.partial(onward, q, h, edge))

    for i, (q, h) in enumerate(order):
        def down_step(n, _, q=q, h=h):
            cs = pl.ds(pl.multiple_of(h * (width // parts) + n * wn, LANES), wn)
            part = jnp.dot(hid[own_rows(q), :], dw[:, cs], preferred_element_type=f32)
            low_, high = part[:half], part[half:]
            om[q, :, cs] = jnp.where(core == 0, low_, high)
            oo[q, :, cs] = jnp.where(core == 0, high, low_).astype(bf16)
            return 0

        lax.fori_loop(0, width // parts // wn, down_step, 0)
        send(oo.at[q, :, strip(h)], orx.at[q, :, strip(h)], t_send.at[q, h], t_recv.at[q, h], mate)
        if i:
            pass_on(*order[i - 1])
    pass_on(*order[-1])

    def take(r, h, buf, sem):
        arrived(buf.at[r, :, strip(h)], sem.at[r, h])
        om[r, :, strip(h)] = om[r, :, strip(h)] + buf[r, :, strip(h)].astype(f32)

    for k in range(RING - 1):
        up, low = RING - 1 - k, k
        for h in range(parts):
            for r, buf, sem, ok in ((up, ubuf, u_recv, z < up), (low, dbuf, d_recv, z > low)):
                @pl.when(ok & ~edge)
                def _(r=r, h=h, buf=buf, sem=sem):
                    take(r, h, buf, sem)
                    onward(r, h, z != r)
    for h in range(parts):
        pl.when(z > 0)(functools.partial(take, z, h, ubuf, u_recv))
        pl.when(z < RING - 1)(functools.partial(take, z, h, dbuf, d_recv))
    ffn = om[z]
    outb[...] = (mixed[...] + scale(ffn, gains[2])).astype(bf16)
    last = local(outb, result)
    for ok, c in sent:
        if ok is None:
            c.wait_send()
        else:
            pl.when(ok)(c.wait_send)
    for zv in range(RING):
        @pl.when(z == zv)
        def _(zv=zv):
            for make in posted[zv]:
                make().wait_send()
    for r in range(RING):
        for h in range(parts):
            there = osend.at[r, :, strip(h)]
            pl.when(z != r)(remote(there, there, o_send.at[r, h], o_send.at[r, h], mate).wait_send)
    last.wait()


def fast_shards(n, resid, queries, keys, values, log_gates, out_gate, out_weight, post_gain,
                pre_gain, ffn_gain, gate_weight, up_weight, down_weight):
    rows, heads_w = queries.shape
    width = resid.shape[1]
    total = rows * PLANE
    heads = heads_w // HD
    group = heads // PLANE
    half = rows // 2
    tiles = gate_weight.shape[1] // LANES
    hw = -(-tiles // PLANE) * LANES
    slab_w = -(-(rows + HD) // LANES) * LANES
    odd = lax.rem(lax.axis_index("sp"), 2) == 1
    slabs = log_gates.T.reshape(PLANE, group, rows)
    fill = lambda left: jnp.pad(slabs, ((0, 0), (0, 8 - group), (left, slab_w - rows - left)))
    slabs = jnp.where(odd, fill(HD), fill(0))
    bf16, f32 = jnp.bfloat16, jnp.float32
    vm = pltpu.VMEM
    gain = lambda g: g.reshape(1, width)
    return pl.pallas_call(
        step_kernel,
        out_shape=jax.ShapeDtypeStruct(resid.shape, resid.dtype),
        in_specs=[ANY] * 13,
        out_specs=ANY,
        scratch_shapes=[
            vm((total, heads_w // PLANE), bf16),
            vm((group * total, LANES), bf16),
            vm(keys.shape, bf16), vm(values.shape, bf16),
            vm((PLANE, rows, LANES), bf16),
            vm((RING, total, LANES), bf16),
            vm((RING, PLANE, 8, slab_w), f32),
            vm((LANES, total), bf16), vm((total, LANES), bf16),
            vm((group * total, 1), f32), vm((group * total, LANES), f32),
            vm((total, heads_w // PLANE), bf16),
            vm((rows, heads_w), bf16), vm((rows, heads_w), bf16),
            vm(out_weight.shape, bf16),
            vm((2, half, width), bf16), vm((half, width), bf16), vm((half, width), bf16),
            vm((half, width), f32), vm((3, 1, width), f32),
            vm((total, width), bf16),
            vm((width, hw), bf16), vm((width, hw), bf16), vm((hw, width), bf16),
            vm((total, hw), f32), vm((total, hw), bf16),
            vm((4, half, width), f32), vm((4, half, width), bf16), vm((4, half, width), bf16),
            vm((4, half, width), bf16), vm((4, half, width), bf16), vm((4, half, width), bf16),
            vm((half, width), bf16),
            DMA((16,)), DMA((3, 3)), DMA((3, PLANE)), DMA((2, 3)), DMA((2, RING)),
            DMA((3,)), DMA((PLANE,)), DMA((3, RING)), DMA((3, n)), DMA((3, RING + 1, 2)), DMA((3, RING)), DMA((3,)),
            DMA, DMA, DMA((10,)), DMA((RING,)), DMA((RING + 1,)), DMA((RING,)),
            DMA((RING, 2)), DMA((RING, 2)), DMA((RING, 2)), DMA((RING, 2)), DMA((RING, 2)),
        ],
        compiler_params=pltpu.CompilerParams(
            collective_id=1, has_side_effects=True, vmem_limit_bytes=62 * 1024 * 1024),
    )(resid, queries, keys, values, slabs, out_gate, out_weight, gain(post_gain), gain(pre_gain),
      gain(ffn_gain), gate_weight, up_weight, down_weight)


def solution(mesh):
    n, cores = mesh.shape["sp"], mesh.shape["tp"]

    def body(*args):
        queries, keys, gate_weight = args[1], args[2], args[10]
        fits = cores == 2 and n == PLANE * RING and keys.shape[1] == PLANE * HD
        fits = fits and queries.shape[1] == 4 * keys.shape[1] and queries.shape[0] % 64 == 0
        fits = fits and gate_weight.shape[1] % LANES == 0 and gate_weight.shape[0] % LANES == 0
        return fast_shards(n, *args) if fits else shards(*args)

    in_specs = (
        P(("sp", "tp"), None),
        P("sp", "tp"),
        P("sp", "tp"),
        P("sp", "tp"),
        P("sp", "tp"),
        P("sp", "tp"),
        P("tp", None),
        P(),
        P(),
        P(),
        P("sp", "tp"),
        P("sp", "tp"),
        P("tp", "sp"),
    )
    out_specs = P(("sp", "tp"), None)
    return jax.shard_map(body, mesh=mesh, in_specs=in_specs, out_specs=out_specs, check_vma=False)
```

```python
import functools

import jax
import jax.numpy as jnp
from jax import lax
from jax.experimental import pallas as pl
from jax.experimental.pallas import tpu as pltpu
from jax.sharding import PartitionSpec as P

HD = 64


EPS = 1e-06
KEY_BLOCK = 512


def rms_scale(rows, gain):
    mean_sq = jnp.mean(rows * rows, axis=-1, keepdims=True)
    return rows * lax.rsqrt(mean_sq + EPS) * gain


def shards(
    resid,
    queries,
    keys,
    values,
    log_gates,
    out_gate,
    out_weight,
    post_gain,
    pre_gain,
    ffn_gain,
    gate_weight,
    up_weight,
    down_weight,
):
    rows = queries.shape[0]
    head_size = HD
    kv_local = keys.shape[1] // head_size
    q_local = queries.shape[1] // head_size
    group = q_local // kv_local
    scale = head_size ** (-0.5)
    offset = lax.axis_index("sp") * rows
    last = offset + rows - 1
    query_pos = offset + jnp.arange(rows, dtype=jnp.int32)
    key_gates = lax.all_gather(log_gates, "sp", axis=0, tiled=True)
    query_blocks = queries.reshape(rows, kv_local, group, head_size)
    query_gates = log_gates.reshape(rows, kv_local, group).transpose(1, 2, 0)

    def key_block(carry, key_rows, value_rows, start):
        count = key_rows.shape[0]

        def compute(state):
            top, denom, accum = state
            scores = (
                jnp.einsum(
                    "tkgd,skd->kgts",
                    query_blocks,
                    key_rows.reshape(count, kv_local, head_size),
                    preferred_element_type=jnp.float32,
                )
                * scale
            )
            gates_here = (
                lax.dynamic_slice_in_dim(key_gates, start, count, 0)
                .reshape(count, kv_local, group)
                .transpose(1, 2, 0)
            )
            scores = scores + query_gates[:, :, :, None] - gates_here[:, :, None, :]
            causal = (start + jnp.arange(count, dtype=jnp.int32))[None, :] <= query_pos[:, None]
            scores = jnp.where(causal[None, None], scores, -jnp.inf)
            new_top = jnp.maximum(top, jnp.max(scores, axis=-1))
            shrink = jnp.exp(top - new_top)
            weights = jnp.exp(scores - new_top[..., None])
            denom = denom * shrink + jnp.sum(weights, axis=-1)
            accum = accum * shrink[..., None] + jnp.einsum(
                "kgts,skd->kgtd",
                weights.astype(jnp.bfloat16),
                value_rows.reshape(count, kv_local, head_size),
                preferred_element_type=jnp.float32,
            )
            return (new_top, denom, accum)

        def keep(state):
            return state

        return lax.cond(start <= last, compute, keep, carry)

    start_state = (
        jnp.full((kv_local, group, rows), -1e30, jnp.float32),
        jnp.zeros((kv_local, group, rows), jnp.float32),
        jnp.zeros((kv_local, group, rows, head_size), jnp.float32),
    )
    carry = start_state
    key_rows = lax.all_gather(keys, "sp", axis=0, tiled=True)
    value_rows = lax.all_gather(values, "sp", axis=0, tiled=True)
    count = key_rows.shape[0]
    blocks = count // KEY_BLOCK
    key_split = key_rows.reshape(blocks, KEY_BLOCK, key_rows.shape[1])
    value_split = value_rows.reshape(blocks, KEY_BLOCK, value_rows.shape[1])

    def advance(state, item):
        index, key_part, value_part = item
        return (key_block(state, key_part, value_part, index * KEY_BLOCK), None)

    carry, _ = lax.scan(
        advance, carry, (jnp.arange(blocks, dtype=jnp.int32), key_split, value_split)
    )
    top, denom, accum = carry
    attended = (accum / denom[..., None]).transpose(2, 0, 1, 3).reshape(rows, q_local * head_size)
    gated = (attended * jax.nn.sigmoid(out_gate.astype(jnp.float32))).astype(jnp.bfloat16)
    projected = lax.psum_scatter(
        jnp.dot(gated, out_weight, preferred_element_type=jnp.float32).astype(jnp.bfloat16),
        "tp",
        scatter_dimension=0,
        tiled=True,
    ).astype(jnp.float32)
    mixed = resid.astype(jnp.float32) + rms_scale(projected, post_gain)
    normed = rms_scale(mixed, pre_gain).astype(jnp.bfloat16)
    normed_all = lax.all_gather(normed, "tp", axis=0, tiled=True)
    gate = jnp.dot(
        normed_all,
        lax.all_gather(gate_weight, "sp", axis=0, tiled=True),
        preferred_element_type=jnp.float32,
    )
    up = jnp.dot(
        normed_all,
        lax.all_gather(up_weight, "sp", axis=0, tiled=True),
        preferred_element_type=jnp.float32,
    )
    hidden = (jax.nn.silu(gate) * up).astype(jnp.bfloat16)
    ffn_partial = jnp.dot(
        hidden,
        lax.all_gather(down_weight, "sp", axis=1, tiled=True),
        preferred_element_type=jnp.float32,
    )
    ffn = lax.psum_scatter(
        ffn_partial.astype(jnp.bfloat16), "tp", scatter_dimension=0, tiled=True
    ).astype(jnp.float32)
    return (mixed + rms_scale(ffn, ffn_gain)).astype(jnp.bfloat16)


LANES = 128
PLANE = 4
RING = 4
MESH = pl.DeviceIdType.MESH
ANY = pl.BlockSpec(memory_space=pl.ANY)
DMA = pltpu.SemaphoreType.DMA


def pick(i, size, unit=1):
    return pl.ds(pl.multiple_of(i * size, unit), size)


def step_kernel(
    resid, queries, keys, values, slabs, out_gate, out_weight, post_gain, pre_gain, ffn_gain,
    gate_weight, up_weight, down_weight, result,
    qb, qx, kin, vin, kvp, kvb, gb, kx, vx, mb, acc, ob, att, og, ow, pb, prx, rs, mixed, gains,
    xall, gw, uw, dw, gacc, hid, om, oo, orx, osend, ubuf, dbuf, outb,
    lsem, a_send, a_recv, z_send, z_recv, b_send, b_recv, w_send, w_recv, r_send, s_send, own_sem,
    p_send, p_recv, x_send, x_recv, m_send, m_recv, o_send, u_recv, d_recv, t_send, t_recv,
):
    me = lax.axis_index("sp")
    core = lax.axis_index("tp")
    p = lax.rem(me, PLANE)
    z = me // PLANE
    base = me - p
    rows, heads_w = queries.shape
    half = rows // 2
    width = resid.shape[1]
    depth = gate_weight.shape[0]
    total = rows * PLANE
    quad = heads_w // PLANE
    group = quad // HD
    hw = gw.shape[1]
    tiles = gate_weight.shape[1] // LANES
    width_of = [min(hw, tiles * LANES - hw * c) for c in range(RING)]
    start_of = [sum(width_of[:c]) for c in range(RING)]
    f32, bf16 = jnp.float32, jnp.bfloat16

    mate = {"tp": 1 - core}
    mates = [p ^ j for j in (1, 2, 3)]
    lines = [z ^ j for j in (1, 2, 3)]
    plane_id = lambda q: {"sp": base + q}
    line_id = lambda c: {"sp": c * PLANE + p}
    peers = [mate] + [plane_id(q) for q in mates] + [line_id(c) for c in lines]
    barrier = pltpu.get_barrier_semaphore()
    for peer in peers:
        pl.semaphore_signal(barrier, inc=1, device_id=peer, device_id_type=MESH)

    def remote(src, dst, send, recv, peer):
        return pltpu.make_async_remote_copy(
            src_ref=src, dst_ref=dst, send_sem=send, recv_sem=recv, device_id=peer, device_id_type=MESH)

    sent = []

    def send(*args, when=None):
        c = remote(*args)
        sent.append((when, c))
        if when is None:
            c.start()
        else:
            pl.when(when)(c.start)

    def arrived(ref, sem):
        remote(ref, ref, sem, sem, mate).wait_recv()

    locals_ = []

    def local(src, dst):
        c = pltpu.make_async_copy(src, dst, lsem.at[len(locals_)])
        c.start()
        locals_.append(c)
        return c

    narrow = width_of[-1]
    if narrow < hw:
        @pl.when(z == RING - 1)
        def _():
            hid[:, narrow:] = jnp.zeros((total, hw - narrow), bf16)
            dw[narrow:, :] = jnp.zeros((hw - narrow, width), bf16)

    k_in = local(keys, kin)
    v_in = local(values, vin)
    cols = lambda q: pick(q, quad, LANES)
    own_rows = lambda q: pick(q, rows, 32)
    own_q = local(queries.at[:, cols(p)], qb.at[own_rows(p), :])
    own_g = local(slabs.at[p], gb.at[z, p])
    wide = lambda c: pl.ds(start_of[c], width_of[c])
    kinds = (
        (lambda c: gate_weight.at[:, wide(c)], lambda s, c: gw.at[pick(s, depth, LANES), :width_of[c]]),
        (lambda c: up_weight.at[:, wide(c)], lambda s, c: uw.at[pick(s, depth, LANES), :width_of[c]]),
        (lambda c: down_weight.at[wide(c), :], lambda s, c: dw.at[:width_of[c], pick(s, depth, LANES)]),
    )
    og_in = local(out_gate, og)
    ow_in = local(out_weight, ow)
    rs_in = local(resid, rs)
    gain_in = [local(g, gains.at[i]) for i, g in enumerate((post_gain, pre_gain, ffn_gain))]
    pl.semaphore_wait(barrier, len(peers))
    for i, q in enumerate(mates):
        send(slabs.at[q], gb.at[z, p], a_send.at[0, i], a_recv.at[0, p], plane_id(q))
    lane = lax.broadcasted_iota(jnp.int32, (rows, LANES), 1)
    k_in.wait()
    v_in.wait()
    for t in range(PLANE // 2):
        ts = pl.ds(t * LANES, LANES)
        kt, vt = kin[:, ts].astype(f32), vin[:, ts].astype(f32)
        kvp[2 * t] = jnp.where(lane < HD, kt, pltpu.roll(vt, HD, 1)).astype(bf16)
        kvp[2 * t + 1] = jnp.where(lane < HD, pltpu.roll(kt, HD, 1), vt).astype(bf16)
    for i, q in enumerate(mates):
        send(kvp.at[q], kvb.at[z, own_rows(p), :], a_send.at[1, i], a_recv.at[1, p], plane_id(q))
    own_kv = local(kvp.at[p], kvb.at[z, own_rows(p), :])
    for i, q in enumerate(mates):
        send(queries.at[:, cols(q)], qb.at[own_rows(p), :], a_send.at[2, i], a_recv.at[2, p], plane_id(q))

    sides = (p ^ 1, p ^ 2)
    posted = [[] for _ in range(RING)]

    def post(zv, make):
        make().start()
        posted[zv].append(make)

    def own(zv, k):
        src, dst = kinds[k]
        pltpu.make_async_copy(src(zv), dst(me, zv), own_sem.at[k]).start()
        for i in range(2):
            post(zv, lambda i=i: remote(
                src(zv), dst(me, zv), r_send.at[k, 0, i], w_recv.at[k, me], plane_id(sides[i])))

    def along(zv, k, c):
        src, dst = kinds[k]
        post(zv, lambda: remote(src(c), dst(me, c), w_send.at[k, c], w_recv.at[k, me], line_id(c)))

    def hop(zv, k, c):
        _, dst = kinds[k]
        there = lambda: dst(c * PLANE + p, zv)
        arrived(there(), w_recv.at[k, c * PLANE + p])
        for i in range(2):
            post(zv, lambda i=i: remote(
                there(), there(), r_send.at[k, 1 + c, i], w_recv.at[k, c * PLANE + p], plane_id(sides[i])))

    def turn(zv, k, c):
        _, dst = kinds[k]
        i = c % 2
        at = lambda: c * PLANE + sides[i]
        arrived(dst(at(), zv), w_recv.at[k, at()])
        post(zv, lambda: remote(
            dst(at(), zv), dst(at(), zv), s_send.at[k, c], w_recv.at[k, at()], plane_id(sides[1 - i])))

    def rest_in(zv, k, c):
        src, dst = kinds[k]
        if c == zv:
            pltpu.make_async_copy(src(zv), dst(me, zv), own_sem.at[k]).wait()
        for s in (c * PLANE + sides[1 - c % 2], c * PLANE + (p ^ 3)):
            arrived(dst(s, zv), w_recv.at[k, s])

    def stage(*table):
        for zv, ops in enumerate(table):
            if ops:
                @pl.when(z == zv)
                def _(zv=zv, ops=ops):
                    for f, *args in ops:
                        with jax.named_scope("_".join([f.__name__, *map(str, args)])):
                            f(zv, *args)

    downs = lambda zv: [(along, k, c) for k in range(3) for c in range(zv - 1, -1, -1)]
    stage(*[[(own, 0), (own, 1), (own, 2)] + downs(zv) for zv in range(RING)])
    own_g.wait()
    own_kv.wait()
    for q in mates:
        arrived(gb.at[z, q], a_recv.at[0, q])
        arrived(kvb.at[z, own_rows(q), :], a_recv.at[1, q])

    def upward(s, d):
        peer = line_id(jnp.minimum(z + 1, RING - 1))
        ok = (z < RING - 1) & (s >= 0)
        s = jnp.maximum(s, 0)
        send(gb.at[s], gb.at[s], z_send.at[0, d], z_recv.at[0, s], peer, when=ok)
        send(kvb.at[s], kvb.at[s], z_send.at[1, d], z_recv.at[1, s], peer, when=ok)

    upward(z, 0)
    stage([(along, 0, 1), (along, 1, 1), (along, 2, 1)], [(along, 0, 2)], [(along, 0, 3)], [])
    def build(s):
        kv = kvb[s].astype(f32)
        g = []
        for t in range(total // LANES):
            g.append(None)
        for q in range(PLANE):
            tile0 = (rows * q) // LANES
            for j in range(gb.shape[3] // LANES):
                part = gb[s, q, :, j * LANES:(j + 1) * LANES]
                if tile0 + j < len(g):
                    g[tile0 + j] = part if g[tile0 + j] is None else g[tile0 + j] + part
        neg = -jnp.concatenate(g, axis=1)
        hi = neg.astype(bf16).astype(f32)
        rest = neg - hi
        mid = rest.astype(bf16).astype(f32)
        low = rest - mid
        pad = jnp.zeros((LANES - HD - 24, total), f32)
        kx[...] = jnp.concatenate([kv.T[:HD], hi, mid, low, pad], axis=0).astype(bf16)
        lk = lax.broadcasted_iota(jnp.int32, (total, LANES), 1)
        vx[...] = jnp.where(lk < HD, 1.0, kv).astype(bf16)
    build(z)
    own_q.wait()
    for q in mates:
        arrived(qb.at[own_rows(q), :], a_recv.at[2, q])
    lq = lax.broadcasted_iota(jnp.int32, (total, LANES), 1)
    for j in range(group):
        t = qb[:, (j // 2) * LANES:(j // 2 + 1) * LANES].astype(f32) * (HD ** -0.5)
        if j % 2:
            t = pltpu.roll(t, HD, 1)
        hot = (lq == HD + j) | (lq == HD + 8 + j) | (lq == HD + 16 + j)
        qx[j * total:(j + 1) * total, :] = jnp.where(lq < HD, t, jnp.where(hot, 1.0, 0.0)).astype(bf16)
    blk = total // 3
    for i in range(3):
        nk = (i + 1) * blk

        def diagonal(h, _, i=i, nk=nk):
            at = [pl.ds(pl.multiple_of((2 * h + e) * total + i * blk, blk), blk) for e in range(2)]
            s = [jnp.dot(qx[r, :], kx[:, :nk], preferred_element_type=f32) for r in at]
            r = lax.broadcasted_iota(jnp.int32, s[0].shape, 0) + i * blk
            c = lax.broadcasted_iota(jnp.int32, s[0].shape, 1)
            s = [jnp.where(c <= r, t, -1e30) for t in s]
            m = [jnp.max(t, axis=1, keepdims=True) for t in s]
            w = [jnp.exp(t - u).astype(bf16) for t, u in zip(s, m)]
            for e, r in enumerate(at):
                mb[r, :] = m[e]
                acc[r, :] = jnp.dot(w[e], vx[:nk, :], preferred_element_type=f32)
            return 0

        lax.fori_loop(0, group // 2, diagonal, 0)

    def full(b, _):
        at = [pl.ds(pl.multiple_of((4 * b + e) * blk, blk), blk) for e in range(4)]
        s = [jnp.dot(qx[r, :], kx[...], preferred_element_type=f32) for r in at]
        old = [mb[r, :] for r in at]
        m = [jnp.maximum(o, jnp.max(t, axis=1, keepdims=True)) for o, t in zip(old, s)]
        w = [jnp.exp(t - u).astype(bf16) for t, u in zip(s, m)]
        for e, r in enumerate(at):
            mb[r, :] = m[e]
            more = jnp.dot(w[e], vx[...], preferred_element_type=f32)
            acc[r, :] = acc[r, :] * jnp.exp(old[e] - m[e]) + more
        return 0

    def plane_step(d, *table):
        @pl.when(z >= d)
        def _():
            arrived(gb.at[z - d], z_recv.at[0, z - d])
            arrived(kvb.at[z - d], z_recv.at[1, z - d])

        if d < RING - 1:
            upward(z - d, d)
        stage(*table)

        @pl.when(z >= d)
        def _():
            build(z - d)
            lax.fori_loop(0, 3 * group // 4, full, 0)
    plane_step(1, [], [(along, 0, 3)], [(hop, 0, 3)], [])
    plane_step(2, [], [(along, 1, 2), (along, 2, 2), (along, 1, 3), (along, 2, 3)], [(hop, 1, 3), (along, 1, 3), (along, 2, 3)], [])
    plane_step(3, [], [], [], [(hop, 0, 2)])
    lane_b = lax.broadcasted_iota(jnp.int32, (blk, LANES), 1)
    for t in range(group // 2):
        def finish(i, _, t=t):
            even = acc[pl.ds(pl.multiple_of(2 * t * total + i * blk, blk), blk), :]
            odd = acc[pl.ds(pl.multiple_of((2 * t + 1) * total + i * blk, blk), blk), :]
            even = even / even[:, :1]
            odd = odd / odd[:, :1]
            both = jnp.where(lane_b < HD, pltpu.roll(even, HD, 1), odd)
            ob[pl.ds(pl.multiple_of(i * blk, blk), blk), t * LANES:(t + 1) * LANES] = both.astype(bf16)
            return 0

        lax.fori_loop(0, 3, finish, 0)
    for i, q in enumerate(mates):
        send(ob.at[own_rows(q), :], att.at[:, cols(p)], b_send.at[i], b_recv.at[p], plane_id(q))
    own_att = local(ob.at[own_rows(p), :], att.at[:, cols(p)])
    stage([(hop, 0, 1), (hop, 0, 3), (hop, 1, 1), (hop, 0, 2)], [(hop, 0, 2), (hop, 0, 3), (hop, 0, 0)],
          [(hop, 0, 1), (hop, 2, 3)], [])
    og_in.wait()
    ow_in.wait()
    rs_in.wait()
    for c in gain_in:
        c.wait()
    own_att.wait()
    for q in mates:
        arrived(att.at[:, cols(q)], b_recv.at[q])
    gated = (att[...].astype(f32) * jax.nn.sigmoid(og[...].astype(f32))).astype(bf16)
    att[...] = gated
    wn = 512

    def project(n, _):
        cs = pick(n, wn, LANES)
        part = jnp.dot(att[...], ow[:, cs], preferred_element_type=f32).astype(bf16)
        pb[0, :, cs] = part[:half]
        pb[1, :, cs] = part[half:]
        return 0

    lax.fori_loop(0, width // wn, project, 0)
    send(pb.at[1 - core], prx, p_send, p_recv, mate)
    arrived(prx, p_recv)

    def scale(v, gain):
        return v * lax.rsqrt(jnp.mean(v * v, axis=-1, keepdims=True) + EPS) * gain

    projected = pb[core].astype(f32) + prx[...].astype(f32)
    mix = rs[...].astype(f32) + scale(projected, gains[0])
    mixed[...] = mix
    parts = 2
    strip = lambda h: pl.ds(h * (width // parts), width // parts)
    rows_of = lambda c, h: pl.ds(pl.multiple_of(c * rows + h * half, 32), half)
    slot = lambda c, e, h: xall.at[rows_of(c, e), strip(h)]
    xall[rows_of(z, core), :] = scale(mix, gains[1]).astype(bf16)
    above = line_id(jnp.minimum(z + 1, RING - 1))
    below = line_id(jnp.maximum(z - 1, 0))
    for h in range(parts):
        mine = slot(z, core, h)
        send(mine, mine, x_send.at[0, h], x_recv.at[z, h], above, when=z < RING - 1)
        send(mine, mine, x_send.at[1, h], x_recv.at[z, h], below, when=z > 0)
        send(mine, mine, m_send.at[0, h], m_recv.at[z, h], mate)
    def rows_from(zv, c):
        for h in range(parts):
            there = lambda h=h: slot(c, core, h)
            arrived(there(), x_recv.at[c, h])
            nxt = zv + 1 if c < zv else zv - 1
            if 0 <= nxt < RING:
                post(zv, lambda there=there, h=h: remote(
                    there(), there(), x_send.at[2 + c, h], x_recv.at[c, h], line_id(nxt)))
            post(zv, lambda there=there, h=h: remote(
                there(), there(), m_send.at[c + 1, h], m_recv.at[c, h], mate))

    turns = lambda k: [(turn, k, c) for c in range(RING)]
    stage(
        [(along, k, c) for k in range(3) for c in (2, 3)]
        + [(hop, 1, 3)] + turns(0) + [(hop, 2, 1), (hop, 1, 2), (hop, 2, 3)] + turns(1)
        + [(hop, 2, 2), (rows_from, 1), (rows_from, 2), (turn, 2, 0), (turn, 2, 1), (rows_from, 3)],
        [(hop, 1, 2), (hop, 1, 0), (hop, 1, 3)] + turns(0) + [(rows_from, 0), (hop, 2, 0)] + turns(1)
        + [(hop, 2, 2), (hop, 2, 3), (rows_from, 2), (turn, 2, 0), (rows_from, 3), (turn, 2, 1)],
        [(hop, 1, 1), (hop, 0, 0)] + turns(0)
        + [(rows_from, 3), (hop, 2, 1), (hop, 1, 0), (rows_from, 1), (hop, 2, 0)] + turns(1)
        + [(rows_from, 0), (turn, 2, 0), (turn, 2, 1)],
        [(hop, 0, 1), (hop, 0, 0)] + turns(0) + [(hop, 1, 2), (hop, 1, 1), (hop, 1, 0), (hop, 2, 2), (hop, 2, 1)]
        + turns(1) + [(hop, 2, 0), (rows_from, 2), (rows_from, 1), (rows_from, 0)],
    )
    for c in range(RING):
        for h in range(parts):
            arrived(slot(c, 1 - core, h), m_recv.at[c, h])

    hn = 256
    hidden_steps = jnp.where(z == RING - 1, pl.cdiv(narrow, hn), hw // hn)
    each = lambda f, k, c: stage(*[[(f, k, c)]] * RING)
    for c in range(RING):
        each(rest_in, 0, c)
    def gate_step(n, _):
        cs = pick(n, hn, LANES)
        gacc[:, cs] = jnp.dot(xall[...], gw[:, cs], preferred_element_type=f32)
        return 0

    lax.fori_loop(0, hidden_steps, gate_step, 0)
    stage([], [], [], [(turn, 2, 0)])
    for c in range(RING):
        each(rest_in, 1, c)
    valid = jnp.where(z < RING - 1, hw, narrow)

    def up_step(n, _):
        cs = pick(n, hn, LANES)
        up = jnp.dot(xall[...], uw[:, cs], preferred_element_type=f32)
        g = gacc[:, cs]
        h = g / (1.0 + jnp.exp(-g)) * up
        unit = lax.broadcasted_iota(jnp.int32, h.shape, 1) + n * hn
        hid[:, cs] = jnp.where(unit < valid, h, 0.0).astype(bf16)
        return 0

    lax.fori_loop(0, hidden_steps, up_step, 0)
    stage([], [], [], [(turn, 2, 1)])
    edge = (z == 0) | (z == RING - 1)
    cut = width // RING
    band = lambda h: pl.ds(h * cut, cut)

    def onward(r, h, when):
        osend[r, :, band(h)] = om[r, :, band(h)].astype(bf16)
        peer = line_id(jnp.clip(jnp.where(r > z, z + 1, z - 1), 0, RING - 1))
        for buf, sem, ok in ((ubuf, u_recv, r > z), (dbuf, d_recv, r < z)):
            src = osend.at[r, :, band(h)]
            c = remote(src, buf.at[r, :, band(h)], o_send.at[r, h], sem.at[r, h], peer)
            pl.when(when & ok)(c.start)

    def pass_on(r, h):
        arrived(orx.at[r, :, band(h)], t_recv.at[r, h])
        om[r, :, band(h)] = om[r, :, band(h)] + orx[r, :, band(h)].astype(f32)
        pl.when(edge & (r != z))(functools.partial(onward, r, h, edge))

    def take(r, h, buf, sem):
        arrived(buf.at[r, :, band(h)], sem.at[r, h])
        om[r, :, band(h)] = om[r, :, band(h)] + buf[r, :, band(h)].astype(f32)

    def down_band(h):
        each(rest_in, 2, h)
        order = [z ^ j for j in (3, 2, 1, 0)]
        for q in order:
            part = jnp.dot(hid[own_rows(q), :], dw[:, band(h)], preferred_element_type=f32)
            low_, high = part[:half], part[half:]
            om[q, :, band(h)] = jnp.where(core == 0, low_, high)
            oo[q, :, band(h)] = jnp.where(core == 0, high, low_).astype(bf16)
            send(oo.at[q, :, band(h)], orx.at[q, :, band(h)], t_send.at[q, h], t_recv.at[q, h], mate)
        for q in order:
            pass_on(q, h)

    def relay_up(zv, h):
        for r in range(RING - 1, zv, -1):
            take(r, h, ubuf, u_recv)
            onward(r, h, z == zv)

    def relay_down(zv, h):
        for r in range(zv):
            take(r, h, dbuf, d_recv)
            onward(r, h, z == zv)

    def chain(h):
        stage(*[
            [] if zv in (0, RING - 1) else
            [(relay_up, h), (relay_down, h)] if zv < RING // 2 else [(relay_down, h), (relay_up, h)]
            for zv in range(RING)])

    each(turn, 2, 2)
    down_band(0)
    each(turn, 2, 3)
    down_band(1)
    chain(0)
    down_band(2)
    chain(1)
    down_band(3)
    chain(2)
    chain(3)
    for h in range(RING):
        pl.when(z > 0)(functools.partial(take, z, h, ubuf, u_recv))
        pl.when(z < RING - 1)(functools.partial(take, z, h, dbuf, d_recv))
    ffn = om[z]
    outb[...] = (mixed[...] + scale(ffn, gains[2])).astype(bf16)
    last = local(outb, result)
    for ok, c in sent:
        if ok is None:
            c.wait_send()
        else:
            pl.when(ok)(c.wait_send)
    for zv in range(RING):
        @pl.when(z == zv)
        def _(zv=zv):
            for make in posted[zv]:
                make().wait_send()
    for r in range(RING):
        for h in range(RING):
            there = osend.at[r, :, band(h)]
            pl.when(z != r)(remote(there, there, o_send.at[r, h], o_send.at[r, h], mate).wait_send)
    last.wait()


def fast_shards(n, resid, queries, keys, values, log_gates, out_gate, out_weight, post_gain,
                pre_gain, ffn_gain, gate_weight, up_weight, down_weight):
    rows, heads_w = queries.shape
    width = resid.shape[1]
    total = rows * PLANE
    heads = heads_w // HD
    group = heads // PLANE
    half = rows // 2
    tiles = gate_weight.shape[1] // LANES
    hw = -(-tiles // PLANE) * LANES
    slab_w = -(-(rows + HD) // LANES) * LANES
    odd = lax.rem(lax.axis_index("sp"), 2) == 1
    slabs = log_gates.T.reshape(PLANE, group, rows)
    fill = lambda left: jnp.pad(slabs, ((0, 0), (0, 8 - group), (left, slab_w - rows - left)))
    slabs = jnp.where(odd, fill(HD), fill(0))
    bf16, f32 = jnp.bfloat16, jnp.float32
    vm = pltpu.VMEM
    gain = lambda g: g.reshape(1, width)
    return pl.pallas_call(
        step_kernel,
        out_shape=jax.ShapeDtypeStruct(resid.shape, resid.dtype),
        in_specs=[ANY] * 13,
        out_specs=ANY,
        scratch_shapes=[
            vm((total, heads_w // PLANE), bf16),
            vm((group * total, LANES), bf16),
            vm(keys.shape, bf16), vm(values.shape, bf16),
            vm((PLANE, rows, LANES), bf16),
            vm((RING, total, LANES), bf16),
            vm((RING, PLANE, 8, slab_w), f32),
            vm((LANES, total), bf16), vm((total, LANES), bf16),
            vm((group * total, 1), f32), vm((group * total, LANES), f32),
            vm((total, heads_w // PLANE), bf16),
            vm((rows, heads_w), bf16), vm((rows, heads_w), bf16),
            vm(out_weight.shape, bf16),
            vm((2, half, width), bf16), vm((half, width), bf16), vm((half, width), bf16),
            vm((half, width), f32), vm((3, 1, width), f32),
            vm((total, width), bf16),
            vm((width, hw), bf16), vm((width, hw), bf16), vm((hw, width), bf16),
            vm((total, hw), f32), vm((total, hw), bf16),
            vm((4, half, width), f32), vm((4, half, width), bf16), vm((4, half, width), bf16),
            vm((4, half, width), bf16), vm((4, half, width), bf16), vm((4, half, width), bf16),
            vm((half, width), bf16),
            DMA((16,)), DMA((3, 3)), DMA((3, PLANE)), DMA((2, 3)), DMA((2, RING)),
            DMA((3,)), DMA((PLANE,)), DMA((3, RING)), DMA((3, n)), DMA((3, RING + 1, 2)), DMA((3, RING)), DMA((3,)),
            DMA, DMA, DMA((10, 2)), DMA((RING, 2)), DMA((RING + 1, 2)), DMA((RING, 2)),
            DMA((RING, RING)), DMA((RING, RING)), DMA((RING, RING)), DMA((RING, RING)), DMA((RING, RING)),
        ],
        compiler_params=pltpu.CompilerParams(
            collective_id=1, has_side_effects=True, vmem_limit_bytes=62 * 1024 * 1024),
    )(resid, queries, keys, values, slabs, out_gate, out_weight, gain(post_gain), gain(pre_gain),
      gain(ffn_gain), gate_weight, up_weight, down_weight)


def solution(mesh):
    n, cores = mesh.shape["sp"], mesh.shape["tp"]

    def body(*args):
        queries, keys, gate_weight = args[1], args[2], args[10]
        fits = cores == 2 and n == PLANE * RING and keys.shape[1] == PLANE * HD
        fits = fits and queries.shape[1] == 4 * keys.shape[1] and queries.shape[0] % 64 == 0
        fits = fits and gate_weight.shape[1] % LANES == 0 and gate_weight.shape[0] % LANES == 0
        return fast_shards(n, *args) if fits else shards(*args)

    in_specs = (
        P(("sp", "tp"), None),
        P("sp", "tp"),
        P("sp", "tp"),
        P("sp", "tp"),
        P("sp", "tp"),
        P("sp", "tp"),
        P("tp", None),
        P(),
        P(),
        P(),
        P("sp", "tp"),
        P("sp", "tp"),
        P("tp", "sp"),
    )
    out_specs = P(("sp", "tp"), None)
    return jax.shard_map(body, mesh=mesh, in_specs=in_specs, out_specs=out_specs, check_vma=False)
```

```python
import functools

import jax
import jax.numpy as jnp
from jax import lax
from jax.experimental import pallas as pl
from jax.experimental.pallas import tpu as pltpu
from jax.sharding import PartitionSpec as P

HD = 64


EPS = 1e-06
KEY_BLOCK = 512


def rms_scale(rows, gain):
    mean_sq = jnp.mean(rows * rows, axis=-1, keepdims=True)
    return rows * lax.rsqrt(mean_sq + EPS) * gain


def shards(
    resid,
    queries,
    keys,
    values,
    log_gates,
    out_gate,
    out_weight,
    post_gain,
    pre_gain,
    ffn_gain,
    gate_weight,
    up_weight,
    down_weight,
):
    rows = queries.shape[0]
    head_size = HD
    kv_local = keys.shape[1] // head_size
    q_local = queries.shape[1] // head_size
    group = q_local // kv_local
    scale = head_size ** (-0.5)
    offset = lax.axis_index("sp") * rows
    last = offset + rows - 1
    query_pos = offset + jnp.arange(rows, dtype=jnp.int32)
    key_gates = lax.all_gather(log_gates, "sp", axis=0, tiled=True)
    query_blocks = queries.reshape(rows, kv_local, group, head_size)
    query_gates = log_gates.reshape(rows, kv_local, group).transpose(1, 2, 0)

    def key_block(carry, key_rows, value_rows, start):
        count = key_rows.shape[0]

        def compute(state):
            top, denom, accum = state
            scores = (
                jnp.einsum(
                    "tkgd,skd->kgts",
                    query_blocks,
                    key_rows.reshape(count, kv_local, head_size),
                    preferred_element_type=jnp.float32,
                )
                * scale
            )
            gates_here = (
                lax.dynamic_slice_in_dim(key_gates, start, count, 0)
                .reshape(count, kv_local, group)
                .transpose(1, 2, 0)
            )
            scores = scores + query_gates[:, :, :, None] - gates_here[:, :, None, :]
            causal = (start + jnp.arange(count, dtype=jnp.int32))[None, :] <= query_pos[:, None]
            scores = jnp.where(causal[None, None], scores, -jnp.inf)
            new_top = jnp.maximum(top, jnp.max(scores, axis=-1))
            shrink = jnp.exp(top - new_top)
            weights = jnp.exp(scores - new_top[..., None])
            denom = denom * shrink + jnp.sum(weights, axis=-1)
            accum = accum * shrink[..., None] + jnp.einsum(
                "kgts,skd->kgtd",
                weights.astype(jnp.bfloat16),
                value_rows.reshape(count, kv_local, head_size),
                preferred_element_type=jnp.float32,
            )
            return (new_top, denom, accum)

        def keep(state):
            return state

        return lax.cond(start <= last, compute, keep, carry)

    start_state = (
        jnp.full((kv_local, group, rows), -1e30, jnp.float32),
        jnp.zeros((kv_local, group, rows), jnp.float32),
        jnp.zeros((kv_local, group, rows, head_size), jnp.float32),
    )
    carry = start_state
    key_rows = lax.all_gather(keys, "sp", axis=0, tiled=True)
    value_rows = lax.all_gather(values, "sp", axis=0, tiled=True)
    count = key_rows.shape[0]
    blocks = count // KEY_BLOCK
    key_split = key_rows.reshape(blocks, KEY_BLOCK, key_rows.shape[1])
    value_split = value_rows.reshape(blocks, KEY_BLOCK, value_rows.shape[1])

    def advance(state, item):
        index, key_part, value_part = item
        return (key_block(state, key_part, value_part, index * KEY_BLOCK), None)

    carry, _ = lax.scan(
        advance, carry, (jnp.arange(blocks, dtype=jnp.int32), key_split, value_split)
    )
    top, denom, accum = carry
    attended = (accum / denom[..., None]).transpose(2, 0, 1, 3).reshape(rows, q_local * head_size)
    gated = (attended * jax.nn.sigmoid(out_gate.astype(jnp.float32))).astype(jnp.bfloat16)
    projected = lax.psum_scatter(
        jnp.dot(gated, out_weight, preferred_element_type=jnp.float32).astype(jnp.bfloat16),
        "tp",
        scatter_dimension=0,
        tiled=True,
    ).astype(jnp.float32)
    mixed = resid.astype(jnp.float32) + rms_scale(projected, post_gain)
    normed = rms_scale(mixed, pre_gain).astype(jnp.bfloat16)
    normed_all = lax.all_gather(normed, "tp", axis=0, tiled=True)
    gate = jnp.dot(
        normed_all,
        lax.all_gather(gate_weight, "sp", axis=0, tiled=True),
        preferred_element_type=jnp.float32,
    )
    up = jnp.dot(
        normed_all,
        lax.all_gather(up_weight, "sp", axis=0, tiled=True),
        preferred_element_type=jnp.float32,
    )
    hidden = (jax.nn.silu(gate) * up).astype(jnp.bfloat16)
    ffn_partial = jnp.dot(
        hidden,
        lax.all_gather(down_weight, "sp", axis=1, tiled=True),
        preferred_element_type=jnp.float32,
    )
    ffn = lax.psum_scatter(
        ffn_partial.astype(jnp.bfloat16), "tp", scatter_dimension=0, tiled=True
    ).astype(jnp.float32)
    return (mixed + rms_scale(ffn, ffn_gain)).astype(jnp.bfloat16)


LANES = 128
PLANE = 4
RING = 4
MESH = pl.DeviceIdType.MESH
ANY = pl.BlockSpec(memory_space=pl.ANY)
DMA = pltpu.SemaphoreType.DMA


def pick(i, size, unit=1):
    return pl.ds(pl.multiple_of(i * size, unit), size)


def step_kernel(
    resid, queries, keys, values, slabs, out_gate, out_weight, post_gain, pre_gain, ffn_gain,
    gate_weight, up_weight, down_weight, result,
    qb, qx, kin, vin, kvp, kvb, gb, kx, vx, mb, acc, ob, att, og, ow, pb, prx, rs, mixed, gains,
    xall, gw, uw, dw, gacc, hid, om, oo, orx, osend, ubuf, dbuf, outb,
    lsem, a_send, a_recv, z_send, z_recv, b_send, b_recv, w_send, w_recv, r_send, s_send, own_sem,
    p_send, p_recv, x_send, x_recv, m_send, m_recv, o_send, u_recv, d_recv, t_send, t_recv,
):
    me = lax.axis_index("sp")
    core = lax.axis_index("tp")
    p = lax.rem(me, PLANE)
    z = me // PLANE
    base = me - p
    rows, heads_w = queries.shape
    half = rows // 2
    width = resid.shape[1]
    depth = gate_weight.shape[0]
    total = rows * PLANE
    quad = heads_w // PLANE
    group = quad // HD
    hw = gw.shape[1]
    tiles = gate_weight.shape[1] // LANES
    width_of = [min(hw, tiles * LANES - hw * c) for c in range(RING)]
    start_of = [sum(width_of[:c]) for c in range(RING)]
    f32, bf16 = jnp.float32, jnp.bfloat16

    mate = {"tp": 1 - core}
    mates = [p ^ j for j in (1, 2, 3)]
    lines = [z ^ j for j in (1, 2, 3)]
    plane_id = lambda q: {"sp": base + q}
    line_id = lambda c: {"sp": c * PLANE + p}
    peers = [mate] + [plane_id(q) for q in mates] + [line_id(c) for c in lines]
    barrier = pltpu.get_barrier_semaphore()
    for peer in peers:
        pl.semaphore_signal(barrier, inc=1, device_id=peer, device_id_type=MESH)

    def remote(src, dst, send, recv, peer):
        return pltpu.make_async_remote_copy(
            src_ref=src, dst_ref=dst, send_sem=send, recv_sem=recv, device_id=peer, device_id_type=MESH)

    sent = []

    def send(*args, when=None):
        c = remote(*args)
        sent.append((when, c))
        if when is None:
            c.start()
        else:
            pl.when(when)(c.start)

    def arrived(ref, sem):
        remote(ref, ref, sem, sem, mate).wait_recv()

    locals_ = []

    def local(src, dst):
        c = pltpu.make_async_copy(src, dst, lsem.at[len(locals_)])
        c.start()
        locals_.append(c)
        return c

    narrow = width_of[-1]
    if narrow < hw:
        @pl.when(z == RING - 1)
        def _():
            hid[:, narrow:] = jnp.zeros((total, hw - narrow), bf16)
            dw[narrow:, :] = jnp.zeros((hw - narrow, width), bf16)

    k_in = local(keys, kin)
    v_in = local(values, vin)
    cols = lambda q: pick(q, quad, LANES)
    own_rows = lambda q: pick(q, rows, 32)
    own_q = local(queries.at[:, cols(p)], qb.at[own_rows(p), :])
    own_g = local(slabs.at[p], gb.at[z, p])
    wide = lambda c: pl.ds(start_of[c], width_of[c])
    kinds = (
        (lambda c: gate_weight.at[:, wide(c)], lambda s, c: gw.at[pick(s, depth, LANES), :width_of[c]]),
        (lambda c: up_weight.at[:, wide(c)], lambda s, c: uw.at[pick(s, depth, LANES), :width_of[c]]),
        (lambda c: down_weight.at[wide(c), :], lambda s, c: dw.at[:width_of[c], pick(s, depth, LANES)]),
    )
    og_in = local(out_gate, og)
    ow_in = local(out_weight, ow)
    rs_in = local(resid, rs)
    gain_in = [local(g, gains.at[i]) for i, g in enumerate((post_gain, pre_gain, ffn_gain))]
    pl.semaphore_wait(barrier, len(peers))
    for i, q in enumerate(mates):
        send(slabs.at[q], gb.at[z, p], a_send.at[0, i], a_recv.at[0, p], plane_id(q))
    lane = lax.broadcasted_iota(jnp.int32, (rows, LANES), 1)
    k_in.wait()
    v_in.wait()
    for t in range(PLANE // 2):
        ts = pl.ds(t * LANES, LANES)
        kt, vt = kin[:, ts].astype(f32), vin[:, ts].astype(f32)
        kvp[2 * t] = jnp.where(lane < HD, kt, pltpu.roll(vt, HD, 1)).astype(bf16)
        kvp[2 * t + 1] = jnp.where(lane < HD, pltpu.roll(kt, HD, 1), vt).astype(bf16)
    for i, q in enumerate(mates):
        send(kvp.at[q], kvb.at[z, own_rows(p), :], a_send.at[1, i], a_recv.at[1, p], plane_id(q))
    own_kv = local(kvp.at[p], kvb.at[z, own_rows(p), :])
    for i, q in enumerate(mates):
        send(queries.at[:, cols(q)], qb.at[own_rows(p), :], a_send.at[2, i], a_recv.at[2, p], plane_id(q))

    sides = (p ^ 1, p ^ 2)
    posted = [[] for _ in range(RING)]

    def post(zv, make):
        make().start()
        posted[zv].append(make)

    def own(zv, k):
        src, dst = kinds[k]
        pltpu.make_async_copy(src(zv), dst(me, zv), own_sem.at[k]).start()
        for i in range(2):
            post(zv, lambda i=i: remote(
                src(zv), dst(me, zv), r_send.at[k, 0, i], w_recv.at[k, me], plane_id(sides[i])))

    def along(zv, k, c):
        src, dst = kinds[k]
        post(zv, lambda: remote(src(c), dst(me, c), w_send.at[k, c], w_recv.at[k, me], line_id(c)))

    def hop(zv, k, c):
        _, dst = kinds[k]
        there = lambda: dst(c * PLANE + p, zv)
        arrived(there(), w_recv.at[k, c * PLANE + p])
        for i in range(2):
            post(zv, lambda i=i: remote(
                there(), there(), r_send.at[k, 1 + c, i], w_recv.at[k, c * PLANE + p], plane_id(sides[i])))

    def turn(zv, k, c):
        _, dst = kinds[k]
        i = c % 2
        at = lambda: c * PLANE + sides[i]
        arrived(dst(at(), zv), w_recv.at[k, at()])
        post(zv, lambda: remote(
            dst(at(), zv), dst(at(), zv), s_send.at[k, c], w_recv.at[k, at()], plane_id(sides[1 - i])))

    def rest_in(zv, k, c):
        src, dst = kinds[k]
        if c == zv:
            pltpu.make_async_copy(src(zv), dst(me, zv), own_sem.at[k]).wait()
        for s in (c * PLANE + sides[1 - c % 2], c * PLANE + (p ^ 3)):
            arrived(dst(s, zv), w_recv.at[k, s])

    def stage(*table):
        for zv, ops in enumerate(table):
            if ops:
                @pl.when(z == zv)
                def _(zv=zv, ops=ops):
                    for f, *args in ops:
                        with jax.named_scope("_".join([f.__name__, *map(str, args)])):
                            f(zv, *args)

    downs = lambda zv: [(along, k, c) for k in range(3) for c in range(zv - 1, -1, -1)]
    ahead = [[(along, 0, 1)], [(along, 0, 2)], [(along, 0, 3)], []]
    stage(*[[(own, 0), (own, 1), (own, 2)] + downs(zv) + ahead[zv] for zv in range(RING)])
    own_g.wait()
    own_kv.wait()
    for q in mates:
        arrived(gb.at[z, q], a_recv.at[0, q])
        arrived(kvb.at[z, own_rows(q), :], a_recv.at[1, q])

    def upward(s, d):
        peer = line_id(jnp.minimum(z + 1, RING - 1))
        ok = (z < RING - 1) & (s >= 0)
        s = jnp.maximum(s, 0)
        send(gb.at[s], gb.at[s], z_send.at[0, d], z_recv.at[0, s], peer, when=ok)
        send(kvb.at[s], kvb.at[s], z_send.at[1, d], z_recv.at[1, s], peer, when=ok)

    upward(z, 0)
    stage([(along, 1, 1), (along, 2, 1)], [(along, 0, 3)], [], [])
    def build(s):
        kv = kvb[s].astype(f32)
        g = []
        for t in range(total // LANES):
            g.append(None)
        for q in range(PLANE):
            tile0 = (rows * q) // LANES
            for j in range(gb.shape[3] // LANES):
                part = gb[s, q, :, j * LANES:(j + 1) * LANES]
                if tile0 + j < len(g):
                    g[tile0 + j] = part if g[tile0 + j] is None else g[tile0 + j] + part
        neg = -jnp.concatenate(g, axis=1)
        hi = neg.astype(bf16).astype(f32)
        rest = neg - hi
        mid = rest.astype(bf16).astype(f32)
        low = rest - mid
        pad = jnp.zeros((LANES - HD - 24, total), f32)
        kx[...] = jnp.concatenate([kv.T[:HD], hi, mid, low, pad], axis=0).astype(bf16)
        lk = lax.broadcasted_iota(jnp.int32, (total, LANES), 1)
        vx[...] = jnp.where(lk < HD, 1.0, kv).astype(bf16)
    build(z)
    own_q.wait()
    for q in mates:
        arrived(qb.at[own_rows(q), :], a_recv.at[2, q])
    lq = lax.broadcasted_iota(jnp.int32, (total, LANES), 1)
    for j in range(group):
        t = qb[:, (j // 2) * LANES:(j // 2 + 1) * LANES].astype(f32) * (HD ** -0.5)
        if j % 2:
            t = pltpu.roll(t, HD, 1)
        hot = (lq == HD + j) | (lq == HD + 8 + j) | (lq == HD + 16 + j)
        qx[j * total:(j + 1) * total, :] = jnp.where(lq < HD, t, jnp.where(hot, 1.0, 0.0)).astype(bf16)
    blk = total // 3
    for i in range(3):
        nk = (i + 1) * blk

        def diagonal(h, _, i=i, nk=nk):
            at = [pl.ds(pl.multiple_of((2 * h + e) * total + i * blk, blk), blk) for e in range(2)]
            s = [jnp.dot(qx[r, :], kx[:, :nk], preferred_element_type=f32) for r in at]
            r = lax.broadcasted_iota(jnp.int32, s[0].shape, 0) + i * blk
            c = lax.broadcasted_iota(jnp.int32, s[0].shape, 1)
            s = [jnp.where(c <= r, t, -1e30) for t in s]
            m = [jnp.max(t, axis=1, keepdims=True) for t in s]
            w = [jnp.exp(t - u).astype(bf16) for t, u in zip(s, m)]
            for e, r in enumerate(at):
                mb[r, :] = m[e]
                acc[r, :] = jnp.dot(w[e], vx[:nk, :], preferred_element_type=f32)
            return 0

        lax.fori_loop(0, group // 2, diagonal, 0)

    def full(b, _):
        at = [pl.ds(pl.multiple_of((4 * b + e) * blk, blk), blk) for e in range(4)]
        s = [jnp.dot(qx[r, :], kx[...], preferred_element_type=f32) for r in at]
        old = [mb[r, :] for r in at]
        m = [jnp.maximum(o, jnp.max(t, axis=1, keepdims=True)) for o, t in zip(old, s)]
        w = [jnp.exp(t - u).astype(bf16) for t, u in zip(s, m)]
        for e, r in enumerate(at):
            mb[r, :] = m[e]
            more = jnp.dot(w[e], vx[...], preferred_element_type=f32)
            acc[r, :] = acc[r, :] * jnp.exp(old[e] - m[e]) + more
        return 0

    def plane_step(d, *table):
        @pl.when(z >= d)
        def _():
            arrived(gb.at[z - d], z_recv.at[0, z - d])
            arrived(kvb.at[z - d], z_recv.at[1, z - d])

        if d < RING - 1:
            upward(z - d, d)
        stage(*table)

        @pl.when(z >= d)
        def _():
            build(z - d)
            lax.fori_loop(0, 3 * group // 4, full, 0)
    plane_step(1, [], [], [(hop, 0, 3)], [])
    plane_step(2, [], [(along, 1, 2), (along, 2, 2), (along, 1, 3), (along, 2, 3)], [(hop, 1, 3), (along, 1, 3), (along, 2, 3)], [])
    plane_step(3, [], [], [], [(hop, 0, 2)])
    lane_b = lax.broadcasted_iota(jnp.int32, (blk, LANES), 1)
    for t in range(group // 2):
        def finish(i, _, t=t):
            even = acc[pl.ds(pl.multiple_of(2 * t * total + i * blk, blk), blk), :]
            odd = acc[pl.ds(pl.multiple_of((2 * t + 1) * total + i * blk, blk), blk), :]
            even = even / even[:, :1]
            odd = odd / odd[:, :1]
            both = jnp.where(lane_b < HD, pltpu.roll(even, HD, 1), odd)
            ob[pl.ds(pl.multiple_of(i * blk, blk), blk), t * LANES:(t + 1) * LANES] = both.astype(bf16)
            return 0

        lax.fori_loop(0, 3, finish, 0)
    for i, q in enumerate(mates):
        send(ob.at[own_rows(q), :], att.at[:, cols(p)], b_send.at[i], b_recv.at[p], plane_id(q))
    own_att = local(ob.at[own_rows(p), :], att.at[:, cols(p)])
    stage([(hop, 0, 1), (hop, 0, 3), (hop, 1, 1), (hop, 0, 2)], [(hop, 0, 2), (hop, 0, 3), (hop, 0, 0)],
          [(hop, 0, 1), (hop, 2, 3)], [])
    og_in.wait()
    ow_in.wait()
    rs_in.wait()
    for c in gain_in:
        c.wait()
    own_att.wait()
    for q in mates:
        arrived(att.at[:, cols(q)], b_recv.at[q])
    gated = (att[...].astype(f32) * jax.nn.sigmoid(og[...].astype(f32))).astype(bf16)
    att[...] = gated
    wn = 512

    def project(n, _):
        cs = pick(n, wn, LANES)
        part = jnp.dot(att[...], ow[:, cs], preferred_element_type=f32).astype(bf16)
        pb[0, :, cs] = part[:half]
        pb[1, :, cs] = part[half:]
        return 0

    lax.fori_loop(0, width // wn, project, 0)
    send(pb.at[1 - core], prx, p_send, p_recv, mate)
    arrived(prx, p_recv)

    def scale(v, gain):
        return v * lax.rsqrt(jnp.mean(v * v, axis=-1, keepdims=True) + EPS) * gain

    projected = pb[core].astype(f32) + prx[...].astype(f32)
    mix = rs[...].astype(f32) + scale(projected, gains[0])
    mixed[...] = mix
    parts = 2
    strip = lambda h: pl.ds(h * (width // parts), width // parts)
    rows_of = lambda c, h: pl.ds(pl.multiple_of(c * rows + h * half, 32), half)
    slot = lambda c, e, h: xall.at[rows_of(c, e), strip(h)]
    xall[rows_of(z, core), :] = scale(mix, gains[1]).astype(bf16)
    above = line_id(jnp.minimum(z + 1, RING - 1))
    below = line_id(jnp.maximum(z - 1, 0))
    for h in range(parts):
        mine = slot(z, core, h)
        send(mine, mine, x_send.at[0, h], x_recv.at[z, h], above, when=z < RING - 1)
        send(mine, mine, x_send.at[1, h], x_recv.at[z, h], below, when=z > 0)
        send(mine, mine, m_send.at[0, h], m_recv.at[z, h], mate)
    def rows_from(zv, c):
        for h in range(parts):
            there = lambda h=h: slot(c, core, h)
            arrived(there(), x_recv.at[c, h])
            nxt = zv + 1 if c < zv else zv - 1
            if 0 <= nxt < RING:
                post(zv, lambda there=there, h=h: remote(
                    there(), there(), x_send.at[2 + c, h], x_recv.at[c, h], line_id(nxt)))
            post(zv, lambda there=there, h=h: remote(
                there(), there(), m_send.at[c + 1, h], m_recv.at[c, h], mate))

    turns = lambda k: [(turn, k, c) for c in range(RING)]
    stage(
        [(along, k, c) for k in range(3) for c in (2, 3)]
        + [(hop, 1, 3)] + turns(0) + [(hop, 2, 1), (hop, 1, 2), (hop, 2, 3)] + turns(1)
        + [(hop, 2, 2), (rows_from, 1), (rows_from, 2), (turn, 2, 0), (turn, 2, 1), (rows_from, 3)],
        [(hop, 1, 2), (hop, 1, 0), (hop, 1, 3)] + turns(0) + [(rows_from, 0), (hop, 2, 0)] + turns(1)
        + [(hop, 2, 2), (hop, 2, 3), (rows_from, 2), (turn, 2, 0), (rows_from, 3), (turn, 2, 1)],
        [(hop, 1, 1), (hop, 0, 0)] + turns(0)
        + [(rows_from, 3), (hop, 2, 1), (hop, 1, 0), (hop, 2, 0), (rows_from, 1)] + turns(1)
        + [(rows_from, 0), (turn, 2, 0), (turn, 2, 1)],
        [(hop, 0, 1), (hop, 0, 0)] + turns(0) + [(hop, 1, 2), (hop, 1, 1), (hop, 1, 0), (hop, 2, 2), (hop, 2, 1)]
        + turns(1) + [(hop, 2, 0), (rows_from, 2), (rows_from, 1), (rows_from, 0)],
    )
    for c in range(RING):
        for h in range(parts):
            arrived(slot(c, 1 - core, h), m_recv.at[c, h])

    hn = 256
    hidden_steps = jnp.where(z == RING - 1, pl.cdiv(narrow, hn), hw // hn)
    each = lambda f, k, c: stage(*[[(f, k, c)]] * RING)
    for c in range(RING):
        each(rest_in, 0, c)
    def gate_step(n, _):
        cs = pick(n, hn, LANES)
        gacc[:, cs] = jnp.dot(xall[...], gw[:, cs], preferred_element_type=f32)
        return 0

    lax.fori_loop(0, hidden_steps, gate_step, 0)
    stage([], [], [], [(turn, 2, 0)])
    for c in range(RING):
        each(rest_in, 1, c)
    valid = jnp.where(z < RING - 1, hw, narrow)

    def up_step(n, _):
        cs = pick(n, hn, LANES)
        up = jnp.dot(xall[...], uw[:, cs], preferred_element_type=f32)
        g = gacc[:, cs]
        h = g / (1.0 + jnp.exp(-g)) * up
        unit = lax.broadcasted_iota(jnp.int32, h.shape, 1) + n * hn
        hid[:, cs] = jnp.where(unit < valid, h, 0.0).astype(bf16)
        return 0

    lax.fori_loop(0, hidden_steps, up_step, 0)
    stage([], [], [], [(turn, 2, 1)])
    edge = (z == 0) | (z == RING - 1)
    cut = width // RING
    band = lambda h: pl.ds(h * cut, cut)

    def onward(r, h, when):
        osend[r, :, band(h)] = om[r, :, band(h)].astype(bf16)
        peer = line_id(jnp.clip(jnp.where(r > z, z + 1, z - 1), 0, RING - 1))
        for buf, sem, ok in ((ubuf, u_recv, r > z), (dbuf, d_recv, r < z)):
            src = osend.at[r, :, band(h)]
            c = remote(src, buf.at[r, :, band(h)], o_send.at[r, h], sem.at[r, h], peer)
            pl.when(when & ok)(c.start)

    def pass_on(r, h):
        arrived(orx.at[r, :, band(h)], t_recv.at[r, h])
        om[r, :, band(h)] = om[r, :, band(h)] + orx[r, :, band(h)].astype(f32)
        pl.when(edge & (r != z))(functools.partial(onward, r, h, edge))

    def take(r, h, buf, sem):
        arrived(buf.at[r, :, band(h)], sem.at[r, h])
        om[r, :, band(h)] = om[r, :, band(h)] + buf[r, :, band(h)].astype(f32)

    def down_band(h):
        each(rest_in, 2, h)
        order = [z ^ j for j in (3, 2, 1, 0)]
        for i, q in enumerate(order):
            part = jnp.dot(hid[own_rows(q), :], dw[:, band(h)], preferred_element_type=f32)
            low_, high = part[:half], part[half:]
            om[q, :, band(h)] = jnp.where(core == 0, low_, high)
            oo[q, :, band(h)] = jnp.where(core == 0, high, low_).astype(bf16)
            send(oo.at[q, :, band(h)], orx.at[q, :, band(h)], t_send.at[q, h], t_recv.at[q, h], mate)
            if i >= 2:
                pass_on(order[i - 2], h)
        pass_on(order[2], h)
        pass_on(order[3], h)

    def relay_up(zv, h):
        for r in range(RING - 1, zv, -1):
            take(r, h, ubuf, u_recv)
            onward(r, h, z == zv)

    def relay_down(zv, h):
        for r in range(zv):
            take(r, h, dbuf, d_recv)
            onward(r, h, z == zv)

    def chain(h):
        stage(*[
            [] if zv in (0, RING - 1) else
            [(relay_up, h), (relay_down, h)] if zv < RING // 2 else [(relay_down, h), (relay_up, h)]
            for zv in range(RING)])

    each(turn, 2, 2)
    down_band(0)
    each(turn, 2, 3)
    down_band(1)
    chain(0)
    down_band(2)
    chain(1)
    down_band(3)
    chain(2)
    chain(3)
    for h in range(RING):
        pl.when(z > 0)(functools.partial(take, z, h, ubuf, u_recv))
        pl.when(z < RING - 1)(functools.partial(take, z, h, dbuf, d_recv))
    ffn = om[z]
    outb[...] = (mixed[...] + scale(ffn, gains[2])).astype(bf16)
    last = local(outb, result)
    for ok, c in sent:
        if ok is None:
            c.wait_send()
        else:
            pl.when(ok)(c.wait_send)
    for zv in range(RING):
        @pl.when(z == zv)
        def _(zv=zv):
            for make in posted[zv]:
                make().wait_send()
    for r in range(RING):
        for h in range(RING):
            there = osend.at[r, :, band(h)]
            pl.when(z != r)(remote(there, there, o_send.at[r, h], o_send.at[r, h], mate).wait_send)
    last.wait()


def fast_shards(n, resid, queries, keys, values, log_gates, out_gate, out_weight, post_gain,
                pre_gain, ffn_gain, gate_weight, up_weight, down_weight):
    rows, heads_w = queries.shape
    width = resid.shape[1]
    total = rows * PLANE
    heads = heads_w // HD
    group = heads // PLANE
    half = rows // 2
    tiles = gate_weight.shape[1] // LANES
    hw = -(-tiles // PLANE) * LANES
    slab_w = -(-(rows + HD) // LANES) * LANES
    odd = lax.rem(lax.axis_index("sp"), 2) == 1
    slabs = log_gates.T.reshape(PLANE, group, rows)
    fill = lambda left: jnp.pad(slabs, ((0, 0), (0, 8 - group), (left, slab_w - rows - left)))
    slabs = jnp.where(odd, fill(HD), fill(0))
    bf16, f32 = jnp.bfloat16, jnp.float32
    vm = pltpu.VMEM
    gain = lambda g: g.reshape(1, width)
    return pl.pallas_call(
        step_kernel,
        out_shape=jax.ShapeDtypeStruct(resid.shape, resid.dtype),
        in_specs=[ANY] * 13,
        out_specs=ANY,
        scratch_shapes=[
            vm((total, heads_w // PLANE), bf16),
            vm((group * total, LANES), bf16),
            vm(keys.shape, bf16), vm(values.shape, bf16),
            vm((PLANE, rows, LANES), bf16),
            vm((RING, total, LANES), bf16),
            vm((RING, PLANE, 8, slab_w), f32),
            vm((LANES, total), bf16), vm((total, LANES), bf16),
            vm((group * total, 1), f32), vm((group * total, LANES), f32),
            vm((total, heads_w // PLANE), bf16),
            vm((rows, heads_w), bf16), vm((rows, heads_w), bf16),
            vm(out_weight.shape, bf16),
            vm((2, half, width), bf16), vm((half, width), bf16), vm((half, width), bf16),
            vm((half, width), f32), vm((3, 1, width), f32),
            vm((total, width), bf16),
            vm((width, hw), bf16), vm((width, hw), bf16), vm((hw, width), bf16),
            vm((total, hw), f32), vm((total, hw), bf16),
            vm((4, half, width), f32), vm((4, half, width), bf16), vm((4, half, width), bf16),
            vm((4, half, width), bf16), vm((4, half, width), bf16), vm((4, half, width), bf16),
            vm((half, width), bf16),
            DMA((16,)), DMA((3, 3)), DMA((3, PLANE)), DMA((2, 3)), DMA((2, RING)),
            DMA((3,)), DMA((PLANE,)), DMA((3, RING)), DMA((3, n)), DMA((3, RING + 1, 2)), DMA((3, RING)), DMA((3,)),
            DMA, DMA, DMA((10, 2)), DMA((RING, 2)), DMA((RING + 1, 2)), DMA((RING, 2)),
            DMA((RING, RING)), DMA((RING, RING)), DMA((RING, RING)), DMA((RING, RING)), DMA((RING, RING)),
        ],
        compiler_params=pltpu.CompilerParams(
            collective_id=1, has_side_effects=True, vmem_limit_bytes=62 * 1024 * 1024),
    )(resid, queries, keys, values, slabs, out_gate, out_weight, gain(post_gain), gain(pre_gain),
      gain(ffn_gain), gate_weight, up_weight, down_weight)


def solution(mesh):
    n, cores = mesh.shape["sp"], mesh.shape["tp"]

    def body(*args):
        queries, keys, gate_weight = args[1], args[2], args[10]
        fits = cores == 2 and n == PLANE * RING and keys.shape[1] == PLANE * HD
        fits = fits and queries.shape[1] == 4 * keys.shape[1] and queries.shape[0] % 64 == 0
        fits = fits and gate_weight.shape[1] % LANES == 0 and gate_weight.shape[0] % LANES == 0
        return fast_shards(n, *args) if fits else shards(*args)

    in_specs = (
        P(("sp", "tp"), None),
        P("sp", "tp"),
        P("sp", "tp"),
        P("sp", "tp"),
        P("sp", "tp"),
        P("sp", "tp"),
        P("tp", None),
        P(),
        P(),
        P(),
        P("sp", "tp"),
        P("sp", "tp"),
        P("tp", "sp"),
    )
    out_specs = P(("sp", "tp"), None)
    return jax.shard_map(body, mesh=mesh, in_specs=in_specs, out_specs=out_specs, check_vma=False)
```

```python
import functools

import jax
import jax.numpy as jnp
from jax import lax
from jax.experimental import pallas as pl
from jax.experimental.pallas import tpu as pltpu
from jax.sharding import PartitionSpec as P

HD = 64


EPS = 1e-06
KEY_BLOCK = 512


def rms_scale(rows, gain):
    mean_sq = jnp.mean(rows * rows, axis=-1, keepdims=True)
    return rows * lax.rsqrt(mean_sq + EPS) * gain


def shards(
    resid,
    queries,
    keys,
    values,
    log_gates,
    out_gate,
    out_weight,
    post_gain,
    pre_gain,
    ffn_gain,
    gate_weight,
    up_weight,
    down_weight,
):
    rows = queries.shape[0]
    head_size = HD
    kv_local = keys.shape[1] // head_size
    q_local = queries.shape[1] // head_size
    group = q_local // kv_local
    scale = head_size ** (-0.5)
    offset = lax.axis_index("sp") * rows
    last = offset + rows - 1
    query_pos = offset + jnp.arange(rows, dtype=jnp.int32)
    key_gates = lax.all_gather(log_gates, "sp", axis=0, tiled=True)
    query_blocks = queries.reshape(rows, kv_local, group, head_size)
    query_gates = log_gates.reshape(rows, kv_local, group).transpose(1, 2, 0)

    def key_block(carry, key_rows, value_rows, start):
        count = key_rows.shape[0]

        def compute(state):
            top, denom, accum = state
            scores = (
                jnp.einsum(
                    "tkgd,skd->kgts",
                    query_blocks,
                    key_rows.reshape(count, kv_local, head_size),
                    preferred_element_type=jnp.float32,
                )
                * scale
            )
            gates_here = (
                lax.dynamic_slice_in_dim(key_gates, start, count, 0)
                .reshape(count, kv_local, group)
                .transpose(1, 2, 0)
            )
            scores = scores + query_gates[:, :, :, None] - gates_here[:, :, None, :]
            causal = (start + jnp.arange(count, dtype=jnp.int32))[None, :] <= query_pos[:, None]
            scores = jnp.where(causal[None, None], scores, -jnp.inf)
            new_top = jnp.maximum(top, jnp.max(scores, axis=-1))
            shrink = jnp.exp(top - new_top)
            weights = jnp.exp(scores - new_top[..., None])
            denom = denom * shrink + jnp.sum(weights, axis=-1)
            accum = accum * shrink[..., None] + jnp.einsum(
                "kgts,skd->kgtd",
                weights.astype(jnp.bfloat16),
                value_rows.reshape(count, kv_local, head_size),
                preferred_element_type=jnp.float32,
            )
            return (new_top, denom, accum)

        def keep(state):
            return state

        return lax.cond(start <= last, compute, keep, carry)

    start_state = (
        jnp.full((kv_local, group, rows), -1e30, jnp.float32),
        jnp.zeros((kv_local, group, rows), jnp.float32),
        jnp.zeros((kv_local, group, rows, head_size), jnp.float32),
    )
    carry = start_state
    key_rows = lax.all_gather(keys, "sp", axis=0, tiled=True)
    value_rows = lax.all_gather(values, "sp", axis=0, tiled=True)
    count = key_rows.shape[0]
    blocks = count // KEY_BLOCK
    key_split = key_rows.reshape(blocks, KEY_BLOCK, key_rows.shape[1])
    value_split = value_rows.reshape(blocks, KEY_BLOCK, value_rows.shape[1])

    def advance(state, item):
        index, key_part, value_part = item
        return (key_block(state, key_part, value_part, index * KEY_BLOCK), None)

    carry, _ = lax.scan(
        advance, carry, (jnp.arange(blocks, dtype=jnp.int32), key_split, value_split)
    )
    top, denom, accum = carry
    attended = (accum / denom[..., None]).transpose(2, 0, 1, 3).reshape(rows, q_local * head_size)
    gated = (attended * jax.nn.sigmoid(out_gate.astype(jnp.float32))).astype(jnp.bfloat16)
    projected = lax.psum_scatter(
        jnp.dot(gated, out_weight, preferred_element_type=jnp.float32).astype(jnp.bfloat16),
        "tp",
        scatter_dimension=0,
        tiled=True,
    ).astype(jnp.float32)
    mixed = resid.astype(jnp.float32) + rms_scale(projected, post_gain)
    normed = rms_scale(mixed, pre_gain).astype(jnp.bfloat16)
    normed_all = lax.all_gather(normed, "tp", axis=0, tiled=True)
    gate = jnp.dot(
        normed_all,
        lax.all_gather(gate_weight, "sp", axis=0, tiled=True),
        preferred_element_type=jnp.float32,
    )
    up = jnp.dot(
        normed_all,
        lax.all_gather(up_weight, "sp", axis=0, tiled=True),
        preferred_element_type=jnp.float32,
    )
    hidden = (jax.nn.silu(gate) * up).astype(jnp.bfloat16)
    ffn_partial = jnp.dot(
        hidden,
        lax.all_gather(down_weight, "sp", axis=1, tiled=True),
        preferred_element_type=jnp.float32,
    )
    ffn = lax.psum_scatter(
        ffn_partial.astype(jnp.bfloat16), "tp", scatter_dimension=0, tiled=True
    ).astype(jnp.float32)
    return (mixed + rms_scale(ffn, ffn_gain)).astype(jnp.bfloat16)


LANES = 128
PLANE = 4
RING = 4
MESH = pl.DeviceIdType.MESH
ANY = pl.BlockSpec(memory_space=pl.ANY)
DMA = pltpu.SemaphoreType.DMA


def pick(i, size, unit=1):
    return pl.ds(pl.multiple_of(i * size, unit), size)


def step_kernel(
    resid, queries, keys, values, slabs, out_gate, out_weight, post_gain, pre_gain, ffn_gain,
    gate_weight, up_weight, down_weight, result,
    qb, qx, kin, vin, kvp, kvb, gb, kx, vx, mb, acc, ob, att, og, ow, pb, prx, rs, mixed, gains,
    xall, gw, uw, dw, gacc, hid, om, oo, orx, osend, ubuf, dbuf, outb,
    lsem, a_send, a_recv, z_send, z_recv, b_send, b_recv, w_send, w_recv, r_send, s_send, own_sem,
    p_send, p_recv, x_send, x_recv, m_send, m_recv, o_send, u_recv, d_recv, t_send, t_recv,
):
    me = lax.axis_index("sp")
    core = lax.axis_index("tp")
    p = lax.rem(me, PLANE)
    z = me // PLANE
    base = me - p
    rows, heads_w = queries.shape
    half = rows // 2
    width = resid.shape[1]
    depth = gate_weight.shape[0]
    total = rows * PLANE
    quad = heads_w // PLANE
    group = quad // HD
    hw = gw.shape[1]
    tiles = gate_weight.shape[1] // LANES
    width_of = [min(hw, tiles * LANES - hw * c) for c in range(RING)]
    start_of = [sum(width_of[:c]) for c in range(RING)]
    f32, bf16 = jnp.float32, jnp.bfloat16

    mate = {"tp": 1 - core}
    mates = [p ^ j for j in (1, 2, 3)]
    lines = [z ^ j for j in (1, 2, 3)]
    plane_id = lambda q: {"sp": base + q}
    line_id = lambda c: {"sp": c * PLANE + p}
    peers = [mate] + [plane_id(q) for q in mates] + [line_id(c) for c in lines]
    barrier = pltpu.get_barrier_semaphore()
    for peer in peers:
        pl.semaphore_signal(barrier, inc=1, device_id=peer, device_id_type=MESH)

    def remote(src, dst, send, recv, peer):
        return pltpu.make_async_remote_copy(
            src_ref=src, dst_ref=dst, send_sem=send, recv_sem=recv, device_id=peer, device_id_type=MESH)

    sent = []

    def send(*args, when=None):
        c = remote(*args)
        sent.append((when, c))
        if when is None:
            c.start()
        else:
            pl.when(when)(c.start)

    def arrived(ref, sem):
        remote(ref, ref, sem, sem, mate).wait_recv()

    locals_ = []

    def local(src, dst):
        c = pltpu.make_async_copy(src, dst, lsem.at[len(locals_)])
        c.start()
        locals_.append(c)
        return c

    narrow = width_of[-1]
    if narrow < hw:
        @pl.when(z == RING - 1)
        def _():
            hid[:, narrow:] = jnp.zeros((total, hw - narrow), bf16)
            dw[narrow:, :] = jnp.zeros((hw - narrow, width), bf16)

    k_in = local(keys, kin)
    v_in = local(values, vin)
    cols = lambda q: pick(q, quad, LANES)
    own_rows = lambda q: pick(q, rows, 32)
    own_q = local(queries.at[:, cols(p)], qb.at[own_rows(p), :])
    own_g = local(slabs.at[p], gb.at[z, p])
    wide = lambda c: pl.ds(start_of[c], width_of[c])
    kinds = (
        (lambda c: gate_weight.at[:, wide(c)], lambda s, c: gw.at[pick(s, depth, LANES), :width_of[c]]),
        (lambda c: up_weight.at[:, wide(c)], lambda s, c: uw.at[pick(s, depth, LANES), :width_of[c]]),
        (lambda c: down_weight.at[wide(c), :], lambda s, c: dw.at[:width_of[c], pick(s, depth, LANES)]),
    )
    og_in = local(out_gate, og)
    ow_in = local(out_weight, ow)
    rs_in = local(resid, rs)
    gain_in = [local(g, gains.at[i]) for i, g in enumerate((post_gain, pre_gain, ffn_gain))]
    pl.semaphore_wait(barrier, len(peers))
    for i, q in enumerate(mates):
        send(slabs.at[q], gb.at[z, p], a_send.at[0, i], a_recv.at[0, p], plane_id(q))
    lane = lax.broadcasted_iota(jnp.int32, (rows, LANES), 1)
    k_in.wait()
    v_in.wait()
    for t in range(PLANE // 2):
        ts = pl.ds(t * LANES, LANES)
        kt, vt = kin[:, ts].astype(f32), vin[:, ts].astype(f32)
        kvp[2 * t] = jnp.where(lane < HD, kt, pltpu.roll(vt, HD, 1)).astype(bf16)
        kvp[2 * t + 1] = jnp.where(lane < HD, pltpu.roll(kt, HD, 1), vt).astype(bf16)
    for i, q in enumerate(mates):
        send(kvp.at[q], kvb.at[z, own_rows(p), :], a_send.at[1, i], a_recv.at[1, p], plane_id(q))
    own_kv = local(kvp.at[p], kvb.at[z, own_rows(p), :])
    for i, q in enumerate(mates):
        send(queries.at[:, cols(q)], qb.at[own_rows(p), :], a_send.at[2, i], a_recv.at[2, p], plane_id(q))

    sides = (p ^ 1, p ^ 2)
    posted = [[] for _ in range(RING)]

    def post(zv, make):
        make().start()
        posted[zv].append(make)

    def own(zv, k):
        src, dst = kinds[k]
        pltpu.make_async_copy(src(zv), dst(me, zv), own_sem.at[k]).start()
        for i in range(2):
            post(zv, lambda i=i: remote(
                src(zv), dst(me, zv), r_send.at[k, 0, i], w_recv.at[k, me], plane_id(sides[i])))

    def along(zv, k, c):
        src, dst = kinds[k]
        post(zv, lambda: remote(src(c), dst(me, c), w_send.at[k, c], w_recv.at[k, me], line_id(c)))

    def hop(zv, k, c):
        _, dst = kinds[k]
        there = lambda: dst(c * PLANE + p, zv)
        arrived(there(), w_recv.at[k, c * PLANE + p])
        for i in range(2):
            post(zv, lambda i=i: remote(
                there(), there(), r_send.at[k, 1 + c, i], w_recv.at[k, c * PLANE + p], plane_id(sides[i])))

    def turn(zv, k, c):
        _, dst = kinds[k]
        i = c // 2
        at = lambda: c * PLANE + sides[i]
        arrived(dst(at(), zv), w_recv.at[k, at()])
        post(zv, lambda: remote(
            dst(at(), zv), dst(at(), zv), s_send.at[k, c], w_recv.at[k, at()], plane_id(sides[1 - i])))

    def rest_in(zv, k, c):
        src, dst = kinds[k]
        if c == zv:
            pltpu.make_async_copy(src(zv), dst(me, zv), own_sem.at[k]).wait()
        for s in (c * PLANE + sides[1 - c // 2], c * PLANE + (p ^ 3)):
            arrived(dst(s, zv), w_recv.at[k, s])

    def stage(*table):
        for zv, ops in enumerate(table):
            if ops:
                @pl.when(z == zv)
                def _(zv=zv, ops=ops):
                    for f, *args in ops:
                        with jax.named_scope("_".join([f.__name__, *map(str, args)])):
                            f(zv, *args)

    downs = lambda zv: [(along, k, c) for k in range(3) for c in range(zv - 1, -1, -1)]
    ahead = [[(along, 0, 1)], [(along, 0, 2)], [(along, 0, 3)], []]
    stage(*[[(own, 0), (own, 1), (own, 2)] + downs(zv) + ahead[zv] for zv in range(RING)])
    own_g.wait()
    own_kv.wait()
    for q in mates:
        arrived(gb.at[z, q], a_recv.at[0, q])
        arrived(kvb.at[z, own_rows(q), :], a_recv.at[1, q])

    def upward(s, d):
        peer = line_id(jnp.minimum(z + 1, RING - 1))
        ok = (z < RING - 1) & (s >= 0)
        s = jnp.maximum(s, 0)
        send(gb.at[s], gb.at[s], z_send.at[0, d], z_recv.at[0, s], peer, when=ok)
        send(kvb.at[s], kvb.at[s], z_send.at[1, d], z_recv.at[1, s], peer, when=ok)

    upward(z, 0)
    stage([(along, 1, 1), (along, 2, 1)], [(along, 0, 3)], [], [])
    def build(s):
        kv = kvb[s].astype(f32)
        g = []
        for t in range(total // LANES):
            g.append(None)
        for q in range(PLANE):
            tile0 = (rows * q) // LANES
            for j in range(gb.shape[3] // LANES):
                part = gb[s, q, :, j * LANES:(j + 1) * LANES]
                if tile0 + j < len(g):
                    g[tile0 + j] = part if g[tile0 + j] is None else g[tile0 + j] + part
        neg = -jnp.concatenate(g, axis=1)
        hi = neg.astype(bf16).astype(f32)
        rest = neg - hi
        mid = rest.astype(bf16).astype(f32)
        low = rest - mid
        pad = jnp.zeros((LANES - HD - 24, total), f32)
        kx[...] = jnp.concatenate([kv.T[:HD], hi, mid, low, pad], axis=0).astype(bf16)
        lk = lax.broadcasted_iota(jnp.int32, (total, LANES), 1)
        vx[...] = jnp.where(lk < HD, 1.0, kv).astype(bf16)
    build(z)
    own_q.wait()
    for q in mates:
        arrived(qb.at[own_rows(q), :], a_recv.at[2, q])
    lq = lax.broadcasted_iota(jnp.int32, (total, LANES), 1)
    for j in range(group):
        t = qb[:, (j // 2) * LANES:(j // 2 + 1) * LANES].astype(f32) * (HD ** -0.5)
        if j % 2:
            t = pltpu.roll(t, HD, 1)
        hot = (lq == HD + j) | (lq == HD + 8 + j) | (lq == HD + 16 + j)
        qx[j * total:(j + 1) * total, :] = jnp.where(lq < HD, t, jnp.where(hot, 1.0, 0.0)).astype(bf16)
    blk = total // 3
    for i in range(3):
        nk = (i + 1) * blk

        def diagonal(h, _, i=i, nk=nk):
            at = [pl.ds(pl.multiple_of((2 * h + e) * total + i * blk, blk), blk) for e in range(2)]
            s = [jnp.dot(qx[r, :], kx[:, :nk], preferred_element_type=f32) for r in at]
            r = lax.broadcasted_iota(jnp.int32, s[0].shape, 0) + i * blk
            c = lax.broadcasted_iota(jnp.int32, s[0].shape, 1)
            s = [jnp.where(c <= r, t, -1e30) for t in s]
            m = [jnp.max(t, axis=1, keepdims=True) for t in s]
            w = [jnp.exp(t - u).astype(bf16) for t, u in zip(s, m)]
            for e, r in enumerate(at):
                mb[r, :] = m[e]
                acc[r, :] = jnp.dot(w[e], vx[:nk, :], preferred_element_type=f32)
            return 0

        lax.fori_loop(0, group // 2, diagonal, 0)

    def full(b, _):
        at = [pl.ds(pl.multiple_of((4 * b + e) * blk, blk), blk) for e in range(4)]
        s = [jnp.dot(qx[r, :], kx[...], preferred_element_type=f32) for r in at]
        old = [mb[r, :] for r in at]
        m = [jnp.maximum(o, jnp.max(t, axis=1, keepdims=True)) for o, t in zip(old, s)]
        w = [jnp.exp(t - u).astype(bf16) for t, u in zip(s, m)]
        for e, r in enumerate(at):
            mb[r, :] = m[e]
            more = jnp.dot(w[e], vx[...], preferred_element_type=f32)
            acc[r, :] = acc[r, :] * jnp.exp(old[e] - m[e]) + more
        return 0

    def plane_step(d, *table):
        @pl.when(z >= d)
        def _():
            arrived(gb.at[z - d], z_recv.at[0, z - d])
            arrived(kvb.at[z - d], z_recv.at[1, z - d])

        if d < RING - 1:
            upward(z - d, d)
        stage(*table)

        @pl.when(z >= d)
        def _():
            build(z - d)
            lax.fori_loop(0, 3 * group // 4, full, 0)
    plane_step(1, [], [], [(hop, 0, 3)], [])
    plane_step(2, [], [(along, 1, 2), (along, 2, 2), (along, 1, 3), (along, 2, 3)], [(hop, 1, 3), (along, 1, 3), (along, 2, 3)], [])
    plane_step(3, [], [], [], [(hop, 0, 2)])
    lane_b = lax.broadcasted_iota(jnp.int32, (blk, LANES), 1)
    for t in range(group // 2):
        def finish(i, _, t=t):
            even = acc[pl.ds(pl.multiple_of(2 * t * total + i * blk, blk), blk), :]
            odd = acc[pl.ds(pl.multiple_of((2 * t + 1) * total + i * blk, blk), blk), :]
            even = even / even[:, :1]
            odd = odd / odd[:, :1]
            both = jnp.where(lane_b < HD, pltpu.roll(even, HD, 1), odd)
            ob[pl.ds(pl.multiple_of(i * blk, blk), blk), t * LANES:(t + 1) * LANES] = both.astype(bf16)
            return 0

        lax.fori_loop(0, 3, finish, 0)
    for i, q in enumerate(mates):
        send(ob.at[own_rows(q), :], att.at[:, cols(p)], b_send.at[i], b_recv.at[p], plane_id(q))
    own_att = local(ob.at[own_rows(p), :], att.at[:, cols(p)])
    stage([(hop, 0, 1), (hop, 0, 3), (hop, 1, 1), (hop, 0, 2)], [(hop, 0, 2), (hop, 0, 3), (hop, 0, 0)],
          [(hop, 0, 1), (hop, 2, 3)], [])
    og_in.wait()
    ow_in.wait()
    rs_in.wait()
    for c in gain_in:
        c.wait()
    own_att.wait()
    for q in mates:
        arrived(att.at[:, cols(q)], b_recv.at[q])
    gated = (att[...].astype(f32) * jax.nn.sigmoid(og[...].astype(f32))).astype(bf16)
    att[...] = gated
    wn = 512

    def project(n, _):
        cs = pick(n, wn, LANES)
        part = jnp.dot(att[...], ow[:, cs], preferred_element_type=f32).astype(bf16)
        pb[0, :, cs] = part[:half]
        pb[1, :, cs] = part[half:]
        return 0

    lax.fori_loop(0, width // wn, project, 0)
    send(pb.at[1 - core], prx, p_send, p_recv, mate)
    arrived(prx, p_recv)

    def scale(v, gain):
        return v * lax.rsqrt(jnp.mean(v * v, axis=-1, keepdims=True) + EPS) * gain

    projected = pb[core].astype(f32) + prx[...].astype(f32)
    mix = rs[...].astype(f32) + scale(projected, gains[0])
    mixed[...] = mix
    parts = 2
    strip = lambda h: pl.ds(h * (width // parts), width // parts)
    rows_of = lambda c, h: pl.ds(pl.multiple_of(c * rows + h * half, 32), half)
    slot = lambda c, e, h: xall.at[rows_of(c, e), strip(h)]
    xall[rows_of(z, core), :] = scale(mix, gains[1]).astype(bf16)
    above = line_id(jnp.minimum(z + 1, RING - 1))
    below = line_id(jnp.maximum(z - 1, 0))
    for h in range(parts):
        mine = slot(z, core, h)
        send(mine, mine, x_send.at[0, h], x_recv.at[z, h], above, when=z < RING - 1)
        send(mine, mine, x_send.at[1, h], x_recv.at[z, h], below, when=z > 0)
        send(mine, mine, m_send.at[0, h], m_recv.at[z, h], mate)
    def rows_from(zv, c):
        for h in range(parts):
            there = lambda h=h: slot(c, core, h)
            arrived(there(), x_recv.at[c, h])
            nxt = zv + 1 if c < zv else zv - 1
            if 0 <= nxt < RING:
                post(zv, lambda there=there, h=h: remote(
                    there(), there(), x_send.at[2 + c, h], x_recv.at[c, h], line_id(nxt)))
            post(zv, lambda there=there, h=h: remote(
                there(), there(), m_send.at[c + 1, h], m_recv.at[c, h], mate))

    turns = lambda k: [(turn, k, c) for c in range(RING)]
    stage(
        [(along, k, c) for k in range(3) for c in (2, 3)]
        + [(hop, 1, 3)] + turns(0) + [(hop, 2, 1), (hop, 1, 2), (hop, 2, 3)] + turns(1)
        + [(hop, 2, 2), (rows_from, 1), (rows_from, 2), (turn, 2, 1), (turn, 2, 3), (rows_from, 3)],
        [(hop, 1, 2), (hop, 1, 0), (hop, 1, 3)] + turns(0) + [(rows_from, 0), (hop, 2, 0)] + turns(1)
        + [(hop, 2, 2), (hop, 2, 3), (rows_from, 2), (turn, 2, 1), (rows_from, 3), (turn, 2, 3)],
        [(hop, 1, 1), (hop, 0, 0)] + turns(0)
        + [(rows_from, 3), (hop, 2, 1), (hop, 1, 0), (hop, 2, 0), (rows_from, 1)] + turns(1)
        + [(rows_from, 0), (turn, 2, 1), (turn, 2, 3)],
        [(hop, 0, 1), (hop, 0, 0)] + turns(0) + [(hop, 1, 2), (hop, 1, 1), (hop, 1, 0), (hop, 2, 2), (hop, 2, 1)]
        + turns(1) + [(hop, 2, 0), (rows_from, 2), (rows_from, 1), (rows_from, 0)],
    )
    for c in range(RING):
        for h in range(parts):
            arrived(slot(c, 1 - core, h), m_recv.at[c, h])

    hn = 256
    hidden_steps = jnp.where(z == RING - 1, pl.cdiv(narrow, hn), hw // hn)
    each = lambda f, k, c: stage(*[[(f, k, c)]] * RING)
    for c in range(RING):
        each(rest_in, 0, c)
    def gate_step(n, _):
        cs = pick(n, hn, LANES)
        gacc[:, cs] = jnp.dot(xall[...], gw[:, cs], preferred_element_type=f32)
        return 0

    lax.fori_loop(0, hidden_steps, gate_step, 0)
    stage([], [], [], [(turn, 2, 1)])
    for c in range(RING):
        each(rest_in, 1, c)
    valid = jnp.where(z < RING - 1, hw, narrow)

    def up_step(n, _):
        cs = pick(n, hn, LANES)
        up = jnp.dot(xall[...], uw[:, cs], preferred_element_type=f32)
        g = gacc[:, cs]
        h = g / (1.0 + jnp.exp(-g)) * up
        unit = lax.broadcasted_iota(jnp.int32, h.shape, 1) + n * hn
        hid[:, cs] = jnp.where(unit < valid, h, 0.0).astype(bf16)
        return 0

    lax.fori_loop(0, hidden_steps, up_step, 0)
    stage([], [], [], [(turn, 2, 3)])
    edge = (z == 0) | (z == RING - 1)
    cut = width // RING
    band = lambda h: pl.ds(h * cut, cut)

    def onward(r, h, when):
        osend[r, :, band(h)] = om[r, :, band(h)].astype(bf16)
        peer = line_id(jnp.clip(jnp.where(r > z, z + 1, z - 1), 0, RING - 1))
        for buf, sem, ok in ((ubuf, u_recv, r > z), (dbuf, d_recv, r < z)):
            src = osend.at[r, :, band(h)]
            c = remote(src, buf.at[r, :, band(h)], o_send.at[r, h], sem.at[r, h], peer)
            pl.when(when & ok)(c.start)

    def pass_on(r, h):
        arrived(orx.at[r, :, band(h)], t_recv.at[r, h])
        om[r, :, band(h)] = om[r, :, band(h)] + orx[r, :, band(h)].astype(f32)
        pl.when(edge & (r != z))(functools.partial(onward, r, h, edge))

    def take(r, h, buf, sem):
        arrived(buf.at[r, :, band(h)], sem.at[r, h])
        om[r, :, band(h)] = om[r, :, band(h)] + buf[r, :, band(h)].astype(f32)

    def down_band(h):
        each(rest_in, 2, h)
        order = [z ^ j for j in (3, 2, 1, 0)]
        for i, q in enumerate(order):
            part = jnp.dot(hid[own_rows(q), :], dw[:, band(h)], preferred_element_type=f32)
            low_, high = part[:half], part[half:]
            om[q, :, band(h)] = jnp.where(core == 0, low_, high)
            oo[q, :, band(h)] = jnp.where(core == 0, high, low_).astype(bf16)
            send(oo.at[q, :, band(h)], orx.at[q, :, band(h)], t_send.at[q, h], t_recv.at[q, h], mate)
            if i >= 2:
                pass_on(order[i - 2], h)
        pass_on(order[2], h)
        pass_on(order[3], h)

    def relay_up(zv, h):
        for r in range(RING - 1, zv, -1):
            take(r, h, ubuf, u_recv)
            onward(r, h, z == zv)

    def relay_down(zv, h):
        for r in range(zv):
            take(r, h, dbuf, d_recv)
            onward(r, h, z == zv)

    def chain(h):
        stage(*[
            [] if zv in (0, RING - 1) else
            [(relay_up, h), (relay_down, h)] if zv < RING // 2 else [(relay_down, h), (relay_up, h)]
            for zv in range(RING)])

    each(turn, 2, 0)
    down_band(1)
    each(turn, 2, 2)
    down_band(3)
    chain(1)
    down_band(0)
    chain(3)
    down_band(2)
    chain(0)
    chain(2)
    for h in range(RING):
        pl.when(z > 0)(functools.partial(take, z, h, ubuf, u_recv))
        pl.when(z < RING - 1)(functools.partial(take, z, h, dbuf, d_recv))
    ffn = om[z]
    outb[...] = (mixed[...] + scale(ffn, gains[2])).astype(bf16)
    last = local(outb, result)
    for ok, c in sent:
        if ok is None:
            c.wait_send()
        else:
            pl.when(ok)(c.wait_send)
    for zv in range(RING):
        @pl.when(z == zv)
        def _(zv=zv):
            for make in posted[zv]:
                make().wait_send()
    for r in range(RING):
        for h in range(RING):
            there = osend.at[r, :, band(h)]
            pl.when(z != r)(remote(there, there, o_send.at[r, h], o_send.at[r, h], mate).wait_send)
    last.wait()


def fast_shards(n, resid, queries, keys, values, log_gates, out_gate, out_weight, post_gain,
                pre_gain, ffn_gain, gate_weight, up_weight, down_weight):
    rows, heads_w = queries.shape
    width = resid.shape[1]
    total = rows * PLANE
    heads = heads_w // HD
    group = heads // PLANE
    half = rows // 2
    tiles = gate_weight.shape[1] // LANES
    hw = -(-tiles // PLANE) * LANES
    slab_w = -(-(rows + HD) // LANES) * LANES
    odd = lax.rem(lax.axis_index("sp"), 2) == 1
    slabs = log_gates.T.reshape(PLANE, group, rows)
    fill = lambda left: jnp.pad(slabs, ((0, 0), (0, 8 - group), (left, slab_w - rows - left)))
    slabs = jnp.where(odd, fill(HD), fill(0))
    bf16, f32 = jnp.bfloat16, jnp.float32
    vm = pltpu.VMEM
    gain = lambda g: g.reshape(1, width)
    return pl.pallas_call(
        step_kernel,
        out_shape=jax.ShapeDtypeStruct(resid.shape, resid.dtype),
        in_specs=[ANY] * 13,
        out_specs=ANY,
        scratch_shapes=[
            vm((total, heads_w // PLANE), bf16),
            vm((group * total, LANES), bf16),
            vm(keys.shape, bf16), vm(values.shape, bf16),
            vm((PLANE, rows, LANES), bf16),
            vm((RING, total, LANES), bf16),
            vm((RING, PLANE, 8, slab_w), f32),
            vm((LANES, total), bf16), vm((total, LANES), bf16),
            vm((group * total, 1), f32), vm((group * total, LANES), f32),
            vm((total, heads_w // PLANE), bf16),
            vm((rows, heads_w), bf16), vm((rows, heads_w), bf16),
            vm(out_weight.shape, bf16),
            vm((2, half, width), bf16), vm((half, width), bf16), vm((half, width), bf16),
            vm((half, width), f32), vm((3, 1, width), f32),
            vm((total, width), bf16),
            vm((width, hw), bf16), vm((width, hw), bf16), vm((hw, width), bf16),
            vm((total, hw), f32), vm((total, hw), bf16),
            vm((4, half, width), f32), vm((4, half, width), bf16), vm((4, half, width), bf16),
            vm((4, half, width), bf16), vm((4, half, width), bf16), vm((4, half, width), bf16),
            vm((half, width), bf16),
            DMA((16,)), DMA((3, 3)), DMA((3, PLANE)), DMA((2, 3)), DMA((2, RING)),
            DMA((3,)), DMA((PLANE,)), DMA((3, RING)), DMA((3, n)), DMA((3, RING + 1, 2)), DMA((3, RING)), DMA((3,)),
            DMA, DMA, DMA((10, 2)), DMA((RING, 2)), DMA((RING + 1, 2)), DMA((RING, 2)),
            DMA((RING, RING)), DMA((RING, RING)), DMA((RING, RING)), DMA((RING, RING)), DMA((RING, RING)),
        ],
        compiler_params=pltpu.CompilerParams(
            collective_id=1, has_side_effects=True, vmem_limit_bytes=62 * 1024 * 1024),
    )(resid, queries, keys, values, slabs, out_gate, out_weight, gain(post_gain), gain(pre_gain),
      gain(ffn_gain), gate_weight, up_weight, down_weight)


def solution(mesh):
    n, cores = mesh.shape["sp"], mesh.shape["tp"]

    def body(*args):
        queries, keys, gate_weight = args[1], args[2], args[10]
        fits = cores == 2 and n == PLANE * RING and keys.shape[1] == PLANE * HD
        fits = fits and queries.shape[1] == 4 * keys.shape[1] and queries.shape[0] % 64 == 0
        fits = fits and gate_weight.shape[1] % LANES == 0 and gate_weight.shape[0] % LANES == 0
        return fast_shards(n, *args) if fits else shards(*args)

    in_specs = (
        P(("sp", "tp"), None),
        P("sp", "tp"),
        P("sp", "tp"),
        P("sp", "tp"),
        P("sp", "tp"),
        P("sp", "tp"),
        P("tp", None),
        P(),
        P(),
        P(),
        P("sp", "tp"),
        P("sp", "tp"),
        P("tp", "sp"),
    )
    out_specs = P(("sp", "tp"), None)
    return jax.shard_map(body, mesh=mesh, in_specs=in_specs, out_specs=out_specs, check_vma=False)
```
